512 devices in a mesh: fs: 64 (over z, y), tp: 8 (over x, core).
Axes of the slice: x: 4, y: 4, z: 16, core: 2. Of those that a mesh axis runs over, the one named last changes fastest.
Arguments:
- tokens: bfloat16 [16384, 2048], P('fs'), may hold values from -6 to 6
- mix_gain: float32 [2048], replicated, may hold values from 0.1 to 1.9
- glu_value: bfloat16 [2048, 2048], P('fs', 'tp'), may hold values from -0.125 to 0.125
- glu_gate: bfloat16 [2048, 2048], P('fs', 'tp'), may hold values from -0.125 to 0.125
- conv_taps: float32 [31, 2048], P(None, 'tp'), may hold values from -2.2 to 2.2, as said below
- chan_gain: float32 [2048], P('tp'), may hold values from 0.1 to 1.9
- mix_out: bfloat16 [2048, 2048], P('tp', 'fs'), may hold values from -0.125 to 0.125
- mlp_gain: float32 [2048], replicated, may hold values from 0.1 to 1.9
- up_weight: bfloat16 [2048, 8192], P('fs', 'tp'), may hold values from -0.125 to 0.125
- down_weight: bfloat16 [8192, 2048], P('tp', 'fs'), may hold values from -0.0625 to 0.0625
Outputs:
- result: bfloat16 [16384, 2048], P('fs')
The draws below stay inside these ranges and needn't reach their ends.
Inputs may be any that keep to these rules, and one draw needn't show every extreme that they name: `conv_taps`: independent entries scaled by fan-in; channels fall into 16 groups of different scale.
All inputs are finite; a program needn't handle non-finite values.
Results may differ from the reference program's by a relative error of at most 0.018.
Values may be sent and summed in bfloat16 or wider, within the bound.
A program may use at most 64 MiB of HBM per device.

```python
import jax
import jax.numpy as jnp
from jax import lax

D = 2048
C = 2048
FF = 8192
WIDTH = 31
LEN = 128
TOKENS = 16384
N_TP = 8


def draw_conv_taps(key, part):
    first, second = jax.random.split(key)
    raw_taps = jnp.clip(jax.random.normal(first, (WIDTH, C), jnp.float32), -4.0, 4.0)
    levels = jnp.exp(jax.random.uniform(second, (16,), jnp.float32, jnp.log(0.3), jnp.log(3.0)))
    return raw_taps * WIDTH ** (-0.5) * jnp.repeat(levels, C // 16)


def block_scale(own_key, dims, shards, smallest, largest):
    def one(position, shards_of):
        heights = jax.random.uniform(jax.random.fold_in(jax.random.fold_in(own_key, 6), position), (shards_of,), jnp.float32, smallest / len(shards), largest / len(shards))
        return jnp.repeat(jnp.exp(heights), dims[position] // shards_of).reshape((-1,) + (1,) * (len(dims) - position - 1))

    level = one(*shards[0])
    for cut in shards[1:]:
        level = level * one(*cut)
    return level


def centred(stream_key, dims, scale, limit, shards=(), held_as=jnp.bfloat16):
    values = jax.random.normal(stream_key, dims, jnp.float32) * scale
    if len(shards) > 0:
        values = block_scale(stream_key, dims, shards, -0.22, 0.18) * values
    return jnp.clip(values, min=-limit, max=limit).astype(held_as)


def setup_inputs(seed: int = 0) -> dict:
    streams_of = jax.random.split(jax.random.key(seed), 11)
    tokens = centred(streams_of[0], (TOKENS, D), 1.0, 6.0, ((0, 64),))
    mix_gain = jnp.clip(1.0 + 0.18 * jax.random.normal(streams_of[1], (D,), jnp.float32), 0.1, 1.9)
    glu_value = centred(streams_of[2], (D, C), D ** -0.5, 0.125, ((0, 64), (1, 8)))
    glu_gate = centred(streams_of[3], (D, C), D ** -0.5, 0.125, ((0, 64), (1, 8)))
    conv_taps = draw_conv_taps(jax.random.fold_in(streams_of[10], 71), 0)
    chan_gain = jnp.clip(1.0 + 0.18 * jax.random.normal(streams_of[5], (C,), jnp.float32), 0.1, 1.9)
    mix_out = centred(streams_of[6], (C, D), C ** -0.5, 0.125, ((0, 8), (1, 64)))
    mlp_gain = jnp.clip(1.0 + 0.18 * jax.random.normal(streams_of[7], (D,), jnp.float32), 0.1, 1.9)
    up_weight = centred(streams_of[8], (D, FF), D ** -0.5, 0.125, ((0, 64), (1, 8)))
    down_weight = centred(streams_of[9], (FF, D), FF ** -0.5, 0.0625, ((0, 8), (1, 64)))
    return {"tokens": tokens, "mix_gain": mix_gain, "glu_value": glu_value, "glu_gate": glu_gate, "conv_taps": conv_taps, "chan_gain": chan_gain, "mix_out": mix_out, "mlp_gain": mlp_gain, "up_weight": up_weight, "down_weight": down_weight}


norm_floor = 0.05

def rms_scale(stream, gain):
    return stream * lax.rsqrt(lax.optimization_barrier(jnp.mean(stream * stream, axis=-1, keepdims=True)) + norm_floor) * gain

def bf16_round(value):
    return lax.optimization_barrier(value.astype(jnp.bfloat16)).astype(jnp.float32)

def depthwise(glu, conv_taps):
    seqs = glu.shape[0] // LEN
    blocks = glu.reshape(seqs, LEN, glu.shape[1]).astype(jnp.float32)
    reach = conv_taps.shape[0] // 2
    padded = jnp.pad(blocks, ((0, 0), (reach, reach), (0, 0)))
    total = jnp.zeros_like(blocks)
    for offset in range(conv_taps.shape[0]):
        total = total + padded[:, offset:offset + LEN] * conv_taps[offset]
    return total.reshape(glu.shape)

def shard_sum(left, right):
    block = left.shape[1] // N_TP
    total = jnp.zeros((left.shape[0], right.shape[1]), jnp.float32)
    for shard in range(N_TP):
        partial_term = jnp.dot(left[:, shard * block:(shard + 1) * block], right[shard * block:(shard + 1) * block], preferred_element_type=jnp.float32)
        total = total + bf16_round(partial_term)
    return total.astype(jnp.bfloat16)

def reference(tokens, mix_gain, glu_value, glu_gate, conv_taps, chan_gain, mix_out, mlp_gain, up_weight, down_weight):
    stream = tokens.astype(jnp.float32)
    normed = rms_scale(stream, mix_gain).astype(jnp.bfloat16)
    values = jnp.dot(normed, glu_value, preferred_element_type=jnp.float32)
    gating = jnp.dot(normed, glu_gate, preferred_element_type=jnp.float32)
    glu = (values * jax.nn.sigmoid(gating)).astype(jnp.bfloat16)
    convolved = depthwise(glu, conv_taps)
    centre = lax.optimization_barrier(jnp.mean(convolved, axis=-1, keepdims=True))
    spread = lax.optimization_barrier(jnp.mean(convolved * convolved, axis=-1, keepdims=True)) - centre * centre
    hidden = jax.nn.silu((convolved - centre) * lax.rsqrt(spread + norm_floor) * chan_gain).astype(jnp.bfloat16)
    mixed = shard_sum(hidden, mix_out)
    resid = stream + mixed.astype(jnp.float32)
    normed_mlp = rms_scale(resid, mlp_gain).astype(jnp.bfloat16)
    active = jnp.square(jax.nn.relu(jnp.dot(normed_mlp, up_weight, preferred_element_type=jnp.float32))).astype(jnp.bfloat16)
    feed = shard_sum(active, down_weight)
    return (resid + feed.astype(jnp.float32)).astype(jnp.bfloat16)
```

```python
import functools

import jax
import jax.numpy as jnp
from jax import lax
from jax.experimental import pallas as pl
from jax.experimental.pallas import tpu as pltpu
from jax.sharding import PartitionSpec as P

MESH = pl.DeviceIdType.MESH
LEN = 128
NY = 4
FLOOR = 0.05
f32, bf16 = jnp.float32, jnp.bfloat16

GROUPS = ((0, 1, 2, 3), (4, 5, 6), (7, 8))


def copy_to(src, dst, ssem, rsem, dev):
    return pltpu.make_async_remote_copy(
        src_ref=src, dst_ref=dst, send_sem=ssem, recv_sem=rsem, device_id=dev, device_id_type=MESH
    )


class Place:
    def __init__(self, nfs):
        self.f, self.t = lax.axis_index("fs"), lax.axis_index("tp")
        self.nz = nfs // NY
        self.half = self.nz // 2
        self.z, self.y = self.f // NY, lax.rem(self.f, NY)

    def blk(self, dz, dy):
        z = lax.rem(self.z + (dz + self.nz), self.nz)
        return z * NY + lax.rem(self.y + (dy + NY), NY)

    def row(self, dz):
        return lax.rem(self.z + (dz + self.nz), self.nz)

    def dev(self, dz, dy):
        return (self.blk(dz, dy), self.t)

    def shifts(self, k):
        if k == 0:
            return (0,)
        return (self.half,) if k == self.half else (-k, k)


class ZFirst:
    def __init__(self, pc, w, ss, zr, yr, hr):
        self.pc, self.w, self.ss, self.zr, self.yr, self.hr = pc, w, ss, zr, yr, hr
        self.n = w.shape[1] // 2

    def part(self, b, which):
        return self.w.at[b, pl.ds(which * self.n, self.n)]

    def send(self, ref, rsem, dev):
        copy_to(ref, ref, self.ss, rsem, dev).start()

    def wait(self, ref, rsem):
        copy_to(ref, ref, self.ss, rsem, self.pc.dev(1, 0)).wait_recv()

    def z(self, k):
        pc, last = self.pc, self.pc.half
        if k == last:
            for d in range(2):
                self.wait(self.part(pc.blk(last, 0), d), self.zr.at[d, k])
        elif k:
            self.wait(self.w.at[pc.blk(-k, 0)], self.zr.at[0, k])
            self.wait(self.w.at[pc.blk(k, 0)], self.zr.at[1, k])
        if k < last:
            for d, way in ((0, 1), (1, -1)):
                b = pc.blk(-way * k, 0)
                ref = self.w.at[b] if k + 1 < last else self.part(b, d)
                self.send(ref, self.zr.at[d, k + 1], pc.dev(way, 0))
        for dz in pc.shifts(k):
            for d, way in ((0, 1), (1, -1)):
                self.send(self.w.at[pc.blk(dz, 0)], self.yr.at[d, k], pc.dev(0, way))

    def f(self, k):
        pc, shifts = self.pc, self.pc.shifts(k)
        for d in range(2):
            self.wait(self.w.at[pl.ds(0, len(shifts))], self.yr.at[d, k])
        for dz in shifts:
            for d, way in ((0, 1), (1, -1)):
                self.send(self.part(pc.blk(dz, -way), d), self.hr.at[d, k], pc.dev(0, way))

    def e(self, k):
        count = len(self.pc.shifts(k))
        for d in range(2):
            if count == 2:
                self.wait(self.w.at[0], self.hr.at[d, k])
            else:
                self.wait(self.part(0, d), self.hr.at[d, k])

    def drain(self):
        whole = self.w.at[pl.ds(0, self.w.shape[0] - 1)]
        copy_to(whole, whole, self.ss, self.zr.at[0, 0], self.pc.dev(1, 0)).wait_send()


class YFirst:
    def __init__(self, pc, w, ss, zr, yr, hr):
        self.pc, self.w, self.ss, self.zr, self.yr, self.hr = pc, w, ss, zr, yr, hr
        self.n = w.shape[1] // 2

    part, send, wait, drain = ZFirst.part, ZFirst.send, ZFirst.wait, ZFirst.drain

    def y0(self):
        for d, way in ((0, 1), (1, -1)):
            self.send(self.w.at[self.pc.f], self.yr.at[d], self.pc.dev(0, way))

    def y1(self):
        pc = self.pc
        for d, way in ((0, 1), (1, -1)):
            b = pc.blk(0, -way)
            self.wait(self.w.at[b], self.yr.at[d])
            self.send(self.part(b, d), self.hr.at[d], pc.dev(0, way))

    def four(self, dz):
        return self.w.at[pl.ds(self.pc.row(dz) * NY, NY)]

    def two(self, dz, which):
        return self.w.at[pl.ds(self.pc.row(dz) * NY + which * 2, 2)]

    def z(self, k):
        pc, last = self.pc, self.pc.half
        if k == 0:
            for d in range(2):
                self.wait(self.part(pc.blk(0, 2), d), self.hr.at[d])
        for d, way in ((0, 1), (1, -1)):
            if k == last:
                self.wait(self.two(last, d), self.zr.at[d, k])
            elif k:
                self.wait(self.four(-way * k), self.zr.at[d, k])
            if k < last:
                ref = self.four(-way * k) if k + 1 < last else self.two(-way * k, d)
                self.send(ref, self.zr.at[d, k + 1], pc.dev(way, 0))


def level(zf, yf, j):
    last = zf.pc.half
    if j <= last:
        zf.z(j)
    if 1 <= j <= last + 1:
        zf.f(j - 1)
    if 2 <= j <= last + 2:
        zf.e(j - 2)
    if j == 0:
        yf.y0()
    if j == 1:
        yf.y1()
    if 2 <= j <= last + 2:
        yf.z(j - 2)


class Exchange:
    def __init__(self, pc, src, dst, sems, spread):
        self.pc, self.src, self.dst, self.sems, self.spread = pc, src, dst, sems, spread

    def start(self):
        pc = self.pc
        nt = self.dst.shape[0]
        for i in range(1, nt):
            to = lax.rem(pc.t + i, nt)
            src = self.src.at[pc.t] if self.spread else self.src.at[to]
            copy_to(src, self.dst.at[pc.t], self.sems.at[0], self.sems.at[1], (pc.f, to)).start()

    def wait(self):
        pc = self.pc
        n = self.dst.shape[0] - 1
        some = self.dst.at[pl.ds(0, n)]
        copy_to(some, some, self.sems.at[0], self.sems.at[1], (pc.f, lax.rem(pc.t + 1, n + 1))).wait_recv()

    def drain(self):
        pc = self.pc
        n = self.dst.shape[0] - 1
        some = self.dst.at[pl.ds(0, n)]
        copy_to(some, some, self.sems.at[0], self.sems.at[1], (pc.f, lax.rem(pc.t + 1, n + 1))).wait_send()


def nt_dot(a, b):
    return lax.dot_general(a, b, (((1,), (1,)), ((), ())), preferred_element_type=f32)


def turned(column):
    return jnp.broadcast_to(column, (column.shape[0], 128)).T[0:1]


def column_of(row):
    return jnp.broadcast_to(row, (128, row.shape[1])).T


def body(
    nfs,
    tok, mix_gain, vw, gw, taps, chan_gain, ow, mlp_gain, uw, dw,
    out,
    x, normed, q1, p1, uq, up, dq, dp,
    padded, conv, stats, mx, rx, nm, resid, aq, ap,
    fx, fr, og,
    load_sem, out_sem,
    q1_s, p1_s, uq_s, up_s, dq_s, dp_s,
    st_sem, mx_sem, nm_sem, fx_sem, og_sem,
):
    pc = Place(nfs)
    nt = rx.shape[0]
    rows = rx.shape[1]
    width = x.shape[1]
    tokens = x.shape[0]
    seqs = tokens // LEN
    last = pc.half
    wq, uc, dc = vw.shape[1], uq.shape[2], dq.shape[2]

    loads = [
        pltpu.make_async_copy(src, dst, load_sem.at[i])
        for i, (src, dst) in enumerate((
            (vw, q1.at[pc.f, :, pl.ds(0, wq)]),
            (gw, q1.at[pc.f, :, pl.ds(wq, wq)]),
            (ow, p1.at[pc.f]),
            (uw.at[:, pl.ds(0, uc)], uq.at[pc.f]),
            (uw.at[:, pl.ds(uc, uw.shape[1] - uc)], up.at[pc.f]),
            (dw.at[:, pl.ds(0, dc)], dq.at[pc.f]),
            (dw.at[:, pl.ds(dc, dw.shape[1] - dc)], dp.at[pc.f]),
            (tok, x),
        ))
    ]
    for load in loads:
        load.start()

    barrier = pltpu.get_barrier_semaphore()
    friends = [pc.dev(1, 0), pc.dev(-1, 0), pc.dev(0, 1), pc.dev(0, -1)]
    friends += [(pc.f, lax.rem(pc.t + i, nt)) for i in range(1, nt)]
    for dev in friends:
        pl.semaphore_signal(barrier, inc=1, device_id=dev, device_id_type=MESH)
    for load in loads:
        load.wait()
    pl.semaphore_wait(barrier, len(friends))

    glu_w, out_w = ZFirst(pc, q1, *q1_s), YFirst(pc, p1, *p1_s)
    up_z, up_y = ZFirst(pc, uq, *uq_s), YFirst(pc, up, *up_s)
    down_z, down_y = ZFirst(pc, dq, *dq_s), YFirst(pc, dp, *dp_s)

    def first(j):
        level(glu_w, out_w, j)

    def second(j):
        level(up_z, up_y, j)

    def third(j):
        level(down_z, down_y, j)

    first(0)
    second(0)

    def norm_rows(i, carry):
        at = pl.ds(pl.multiple_of(i * 32, 32), 32)
        s = x[at].astype(f32)
        scale = lax.rsqrt(jnp.mean(s * s, axis=-1, keepdims=True) + FLOOR)
        normed[at] = (s * scale * mix_gain[...]).astype(bf16)
        return carry

    lax.fori_loop(0, tokens // 32, norm_rows, 0)

    done = 1
    for j in range(1, last + 3):
        first(j)
        if j % 2 == 0 and done < 5:
            second(done)
            done += 1

    n_all = normed[...]
    values = jnp.dot(n_all, q1[:, :, pl.ds(0, wq)].reshape(width, wq), preferred_element_type=f32)
    gating = jnp.dot(n_all, q1[:, :, pl.ds(wq, wq)].reshape(width, wq), preferred_element_type=f32)
    glu = (values * jax.nn.sigmoid(gating)).astype(bf16).astype(f32)
    reach = taps.shape[0] // 2
    halves = wq // 128
    zeros = jnp.zeros((16, 128), f32)
    for h in range(halves):
        for s in range(seqs):
            padded[h, s, pl.ds(0, 16)] = zeros
            padded[h, s, pl.ds(16, LEN)] = glu[s * LEN : (s + 1) * LEN, h * 128 : (h + 1) * 128]
            padded[h, s, pl.ds(16 + LEN, 16)] = zeros
    second(done)
    third(0)

    for h in range(halves):
        for s in range(seqs):
            total = jnp.zeros((LEN, 128), f32)
            for o in range(taps.shape[0]):
                total = total + padded[h, s, pl.ds(16 - reach + o, LEN)] * taps[pl.ds(o, 1), pl.ds(h * 128, 128)]
            conv[h, pl.ds(s * LEN, LEN)] = total
    sums = sum(jnp.sum(conv[h], axis=-1, keepdims=True) for h in range(halves))
    squares = sum(jnp.sum(conv[h] * conv[h], axis=-1, keepdims=True) for h in range(halves))
    stats[pc.t, pl.ds(0, 1)] = turned(sums)
    stats[pc.t, pl.ds(1, 1)] = turned(squares)
    second(done + 1)
    stat_x = Exchange(pc, stats, stats, st_sem, True)
    stat_x.start()
    third(1)
    stat_x.wait()

    all_stats = jnp.sum(stats[...], axis=0)
    channels = wq * nt
    centre = column_of(all_stats[0:1]) / channels
    spread = column_of(all_stats[1:2]) / channels - centre * centre
    scale = lax.rsqrt(spread + FLOOR)
    hidden = []
    for h in range(halves):
        v = (conv[h] - centre) * scale * chan_gain[:, h * 128 : (h + 1) * 128]
        hidden.append((v * jax.nn.sigmoid(v)).astype(bf16))
    hidden = jnp.concatenate(hidden, axis=1)
    for c in range(width // 256):
        w = p1[pl.ds(c * 8, 8)].reshape(256, wq)
        mx[:, :, pl.ds(c * 256, 256)] = nt_dot(hidden, w).astype(bf16).reshape(nt, rows, 256)
    second(done + 2)
    mix_x = Exchange(pc, mx, rx, mx_sem, False)
    mix_x.start()
    third(2)
    second(done + 3)
    third(3)
    mix_x.wait()

    rx[pc.t] = mx[pc.t]
    mixed = rx[0].astype(f32)
    for i in range(1, nt):
        mixed = mixed + rx[i].astype(f32)
    own = x[pl.ds(pl.multiple_of(pc.t * rows, rows), rows)].astype(f32)
    res = own + mixed.astype(bf16).astype(f32)
    resid[...] = res
    scale = lax.rsqrt(jnp.mean(res * res, axis=-1, keepdims=True) + FLOOR)
    nm[pc.t] = (res * scale * mlp_gain[...]).astype(bf16)
    second(done + 4)
    norm_x = Exchange(pc, nm, nm, nm_sem, True)
    norm_x.start()
    third(4)
    second(done + 5)
    third(5)
    norm_x.wait()

    n_mlp = nm[...].reshape(tokens, width)
    for src, dst in ((uq, aq), (up, ap)):
        cols = src.shape[2]
        for c in range(0, cols, 256):
            n = min(256, cols - c)
            a = jnp.dot(n_mlp, src[:, :, pl.ds(c, n)].reshape(width, n), preferred_element_type=f32)
            a = jnp.maximum(a, 0.0)
            dst[:, pl.ds(c, n)] = (a * a).astype(bf16)

    act_q, act_p = aq[...], ap[...]

    def slots(g):
        return [dz for k in GROUPS[g] for dz in pc.shifts(k)]

    def multiply(g):
        for s, dz in enumerate(slots(g)):
            b = pl.ds(pc.row(dz) * NY, NY)
            part = nt_dot(act_q, dq[b].reshape(128, dc)) + nt_dot(act_p, dp[b].reshape(128, dp.shape[2]))
            fx[g][:, :, pl.ds(s * 128, 128)] = part.astype(bf16).reshape(nt, rows, 128)

    sums_x = [Exchange(pc, fx[g], fr[g], fx_sem.at[g], False) for g in range(len(GROUPS))]
    done_x = [Exchange(pc, og[g], og[g], og_sem.at[g], True) for g in range(len(GROUPS))]

    def finish(g):
        sums_x[g].wait()
        fr[g][pc.t] = fx[g][pc.t]
        for s, dz in enumerate(slots(g)):
            at = pl.ds(s * 128, 128)
            feed = fr[g][0, :, at].astype(f32)
            for i in range(1, nt):
                feed = feed + fr[g][i, :, at].astype(f32)
            to = pl.ds(pl.multiple_of(pc.row(dz) * 128, 128), 128)
            og[g][pc.t, :, at] = (resid[:, to] + feed.astype(bf16).astype(f32)).astype(bf16)

    def write(g):
        done_x[g].wait()
        for s, dz in enumerate(slots(g)):
            to = pl.ds(pl.multiple_of(pc.row(dz) * 128, 128), 128)
            pltpu.make_async_copy(og[g].at[:, :, pl.ds(s * 128, 128)], out.at[:, :, to], out_sem).start()

    multiply(0)
    third(6)
    sums_x[0].start()
    third(7)
    third(8)
    multiply(1)
    sums_x[1].start()
    finish(0)
    done_x[0].start()
    third(9)
    third(10)
    multiply(2)
    sums_x[2].start()
    finish(1)
    done_x[1].start()
    write(0)
    finish(2)
    done_x[2].start()
    write(1)
    write(2)

    for stream in (glu_w, out_w, up_z, up_y, down_z, down_y):
        stream.drain()
    for x_ in [stat_x, mix_x, norm_x, *sums_x, *done_x]:
        x_.drain()
    pltpu.make_async_copy(out, out, out_sem).wait()


def layer(nfs, nt, tok, mix_gain, vw, gw, taps, chan_gain, ow, mlp_gain, uw, dw):
    tokens, width = tok.shape
    k_rows, wq = vw.shape
    ff = uw.shape[1]
    rows = tokens // nt
    last = nfs // NY // 2
    uc = ff * 5 // 8
    dma = pltpu.SemaphoreType.DMA
    one = lambda: [dma(()), dma((2, last + 1)), dma((2, last + 1)), dma((2, last + 1))]
    other = lambda: [dma(()), dma((2, last + 1)), dma((2,)), dma((2,))]
    widths = [sum(1 if k in (0, last) else 2 for k in g) * 128 for g in GROUPS]
    pieces = lambda: [pltpu.VMEM((nt, rows, w), bf16) for w in widths]
    block = lambda c: pltpu.VMEM((nfs, k_rows, c), bf16)
    hbm, vmem = pl.BlockSpec(memory_space=pl.ANY), pl.BlockSpec(memory_space=pltpu.VMEM)
    scratch = [
        pltpu.VMEM((tokens, width), bf16),
        pltpu.VMEM((tokens, width), bf16),
        block(2 * wq), block(wq), block(uc), block(ff - uc), block(uc), block(ff - uc),
        pltpu.VMEM((wq // 128, tokens // LEN, LEN + 32, 128), f32),
        pltpu.VMEM((wq // 128, tokens, 128), f32),
        pltpu.VMEM((nt, 2, tokens), f32),
        pltpu.VMEM((nt, rows, width), bf16),
        pltpu.VMEM((nt, rows, width), bf16),
        pltpu.VMEM((nt, rows, width), bf16),
        pltpu.VMEM((rows, width), f32),
        pltpu.VMEM((tokens, uc), bf16),
        pltpu.VMEM((tokens, ff - uc), bf16),
        pieces(), pieces(), pieces(),
        dma((8,)), dma(()),
        one(), other(), one(), other(), one(), other(),
        dma((2,)), dma((2,)), dma((2,)), dma((len(GROUPS), 2)), dma((len(GROUPS), 2)),
    ]
    done = pl.pallas_call(
        functools.partial(body, nfs),
        out_shape=jax.ShapeDtypeStruct((nt, rows, width), bf16),
        in_specs=[hbm, vmem, hbm, hbm, vmem, vmem, hbm, vmem, hbm, hbm],
        out_specs=hbm,
        scratch_shapes=scratch,
        compiler_params=pltpu.CompilerParams(
            collective_id=0, has_side_effects=True, vmem_limit_bytes=56 * 1024 * 1024
        ),
        name="layer",
    )(
        tok, mix_gain.reshape(1, -1), vw, gw, taps, chan_gain.reshape(1, -1), ow.T,
        mlp_gain.reshape(1, -1), uw, dw.T,
    )
    return done.reshape(tokens, width)


def solution(mesh):
    in_specs = (
        P("fs", None), P(), P("fs", "tp"), P("fs", "tp"), P(None, "tp"),
        P("tp"), P("tp", "fs"), P(), P("fs", "tp"), P("tp", "fs"),
    )
    nfs, nt = mesh.shape["fs"], mesh.shape["tp"]
    return jax.shard_map(
        functools.partial(layer, nfs, nt), mesh=mesh, in_specs=in_specs,
        out_specs=P("fs", None), check_vma=False,
    )
```

```python
import functools

import jax
import jax.numpy as jnp
from jax import lax
from jax.experimental import pallas as pl
from jax.experimental.pallas import tpu as pltpu
from jax.sharding import PartitionSpec as P

MESH = pl.DeviceIdType.MESH
LEN = 128
NY = 4
FLOOR = 0.05
f32, bf16 = jnp.float32, jnp.bfloat16

ORDER = (
    "v.y0", "g.z0", "u.z0", "d.y0", "e.y0", "o.y0", "o.z0", "d.z0", "g.y0", "u.y0", "g.z1", "v.y1", "g.y1", "g.y2",
    "o.y1", "g.z2", "u.y1", "e.y1", "u.f0", "g.f0", "o.z1", "o.z2", "o.f0", "g.z3", "g.y3", "d.z1", "g.z4", "u.f1",
    "u.z1", "o.y3", "o.y4", "v.z01", "o.z4", "o.z3", "d.y2", "g.f1", "v.z00", "g.y5", "d.z2", "u.z2", "g.z6", "g.z5",
    "o.y2", "v.z11", "g.y6", "d.f0", "g.y4", "o.f4", "d.z3", "o.z6", "v.z10", "o.z5", "g.f2", "d.f2", "g.y8", "u.z3",
    "o.f1", "g.y7", "o.y6", "e.z01", "o.y5", "v.z20", "e.z00", "N", "g.f4", "u.z4", "g.f3", "e.z11", "g.f6", "g.f5",
    "o.f2", "o.y8", "o.f6", "d.z4", "d.y3", "o.y7", "e.z10", "u.z5", "o.f5", "o.f3", "v.z21", "u.y5", "v.z30", "u.y4",
    "G", "e.z21", "C", "u.y2", "e.z20", "v.z31", "v.z40", "H", "u.y3", "d.y1", "d.z5", "u.z6", "I", "B", "v.z41",
    "v.z50", "u.f4", "d.y5", "d.f3", "u.z7", "e.z30", "u.y7", "u.y6", "v.z51", "e.z31", "d.z6", "e.z40", "v.z60",
    "u.y8", "u.f5", "E", "e.z41", "d.y4", "u.f2", "v.z61", "e.z50", "u.f6", "u.f3", "d.f1", "e.z51", "v.z71", "v.z70",
    "d.f5", "d.z7", "e.z60", "d.f4", "d.y6", "L", "e.z61", "d.y7", "U", "M0", "d.f6", "d.y8", "M1", "e.z70", "e.z71",
    "S0", "S1", "M2", "M3", "S2", "S3", "F0", "F1", "F3", "F2", "R0", "W0", "R3", "R1", "R2", "W1", "W3", "W2",
)
GROUPS = ((0, 1, 2, 3), (4, 5), (6, 7), (8,))
DIRECT = 7


def copy_to(src, dst, ssem, rsem, dev):
    return pltpu.make_async_remote_copy(
        src_ref=src, dst_ref=dst, send_sem=ssem, recv_sem=rsem, device_id=dev, device_id_type=MESH
    )


class Place:
    def __init__(self, nfs, nt):
        self.f, self.t = lax.axis_index("fs"), lax.axis_index("tp")
        self.nz = nfs // NY
        self.half = self.nz // 2
        self.z, self.y = self.f // NY, lax.rem(self.f, NY)
        self.nx = nt // 2
        self.x, self.c = self.t // 2, lax.rem(self.t, 2)

    def row(self, dz):
        return lax.rem(self.z + (dz + self.nz), self.nz)

    def blk(self, dz, dy):
        return self.row(dz) * NY + lax.rem(self.y + (dy + NY), NY)

    def dev(self, dz, dy):
        return (self.blk(dz, dy), self.t)

    def along_x(self, i):
        x = lax.rem(self.x + i, self.nx)
        return x, (self.f, x * 2 + self.c)

    def partner(self):
        return (self.f, self.x * 2 + 1 - self.c)

    def shifts(self, k):
        if k == 0:
            return (0,)
        return (self.half,) if k == self.half else (-k, k)


class Stream:
    def __init__(self, pc, w, sems, loads, stride):
        self.pc, self.w, self.loads, self.stride = pc, w, loads, stride
        self.ss, self.zr, self.yr, self.hr = sems
        self.n = w.shape[1] // 2
        self.came = set()

    def part(self, b, which):
        return self.w.at[b, pl.ds(which * self.n, self.n)]

    def send(self, ref, rsem, dev):
        copy_to(ref, ref, self.ss, rsem, dev).start()

    def await_(self, ref, rsem):
        copy_to(ref, ref, self.ss, rsem, self.pc.dev(1, 0)).wait_recv()

    def need(self, *key):
        if key not in self.came:
            self.came.add(key)
            self.arrive(*key)

    def own(self):
        if "own" not in self.came:
            self.came.add("own")
            for load in self.loads:
                load.wait()

    def drain(self):
        whole = self.w.at[pl.ds(0, self.w.shape[0] - 1)]
        copy_to(whole, whole, self.ss, self.yr.at[0, 0], self.pc.dev(1, 0)).wait_send()


class ZFirst(Stream):
    def arrive(self, what, k):
        pc = self.pc
        for d in range(2):
            if what == "z":
                b = pc.blk(k if d else -k, 0)
                self.await_(self.part(b, d) if k == pc.half else self.w.at[b], self.zr.at[d, k])
            elif what == "y":
                self.await_(self.w.at[pl.ds(0, len(pc.shifts(k)))], self.yr.at[d, k])
            elif k >= DIRECT:
                if d == 0:
                    self.await_(self.w.at[pl.ds(0, len(pc.shifts(k)))], self.hr.at[0, k])
            else:
                self.await_(self.w.at[0] if len(pc.shifts(k)) == 2 else self.part(0, d), self.hr.at[d, k])

    def all_of(self, k):
        self.own()
        for what in "zyh" if k else "yh":
            self.need(what, k)

    def ready(self, k):
        if k:
            self.need("z", k)
        else:
            self.own()

    def z(self, k):
        pc = self.pc
        self.ready(k)
        for step in range(1, self.stride + 1) if k == 0 else (self.stride,):
            for d, way in ((0, 1), (1, -1)):
                b = pc.blk(-way * k, 0)
                ref = self.part(b, d) if k + step == pc.half else self.w.at[b]
                self.send(ref, self.zr.at[d, k + step], pc.dev(way * step, 0))

    def y(self, k):
        pc = self.pc
        self.ready(k)
        for dz in pc.shifts(k):
            ref = self.w.at[pc.blk(dz, 0)]
            for d, way in ((0, 1), (1, -1)):
                self.send(ref, self.yr.at[d, k], pc.dev(0, way))
            if k >= DIRECT:
                self.send(ref, self.hr.at[0, k], pc.dev(0, 2))

    def f(self, k):
        pc = self.pc
        self.need("y", k)
        for dz in pc.shifts(k):
            for d, way in ((0, 1), (1, -1)):
                self.send(self.part(pc.blk(dz, -way), d), self.hr.at[d, k], pc.dev(0, way))


class YFirst(Stream):
    def two(self, dz, h):
        return self.w.at[pl.ds(self.pc.row(dz) * NY + h * 2, 2)]

    def arrive(self, what, k, h=0):
        pc = self.pc
        for d, way in ((0, 1), (1, -1)):
            if what == "y":
                self.await_(self.w.at[pc.blk(0, -way)], self.yr.at[d, 0])
            elif what == "h":
                self.await_(self.part(pc.blk(0, 2), d), self.hr.at[d, 0])
            elif k < pc.half or d == h:
                self.await_(self.two(-way * k, h), self.zr.at[d, k, h])

    def all_of(self, k):
        self.own()
        if k:
            for h in range(2):
                self.need("z", k, h)
        else:
            self.need("y", 0)
            self.need("h", 0)

    def y(self, k):
        pc = self.pc
        if k == 0:
            self.own()
        else:
            self.need("y", 0)
        for d, way in ((0, 1), (1, -1)):
            if k == 0:
                self.send(self.w.at[pc.f], self.yr.at[d, 0], pc.dev(0, way))
            else:
                self.send(self.part(pc.blk(0, -way), d), self.hr.at[d, 0], pc.dev(0, way))

    def z(self, kh):
        pc = self.pc
        k, h = kh // 10, kh % 10
        if k:
            self.need("z", k, h)
        else:
            self.all_of(0)
        for d, way in ((0, 1), (1, -1)):
            if k + 1 < pc.half or d == h:
                self.send(self.two(-way * k, h), self.zr.at[d, k + 1, h], pc.dev(way, 0))


class PairSum:
    def __init__(self, pc, other, got, mine, came, sems):
        self.pc, self.other, self.got, self.mine, self.came, self.sems = pc, other, got, mine, came, sems

    def swap(self):
        return copy_to(self.other, self.got, self.sems.at[0], self.sems.at[1], self.pc.partner())

    def spread(self):
        pc = self.pc
        for i in range(1, pc.nx):
            x, dev = pc.along_x(i)
            copy_to(self.mine.at[x], self.came.at[pc.x], self.sems.at[2], self.sems.at[3], dev).start()

    def three(self):
        some = self.came.at[pl.ds(0, self.pc.nx - 1)]
        return copy_to(some, some, self.sems.at[2], self.sems.at[3], self.pc.partner())


class PairGather:
    def __init__(self, pc, buf, sems):
        self.pc, self.buf, self.sems = pc, buf, sems

    def own(self):
        pc = self.pc
        ref = self.buf.at[pc.x, pc.c]
        return copy_to(ref, ref, self.sems.at[2], self.sems.at[3], pc.partner())

    def start(self):
        pc = self.pc
        ref = self.buf.at[pc.x, pc.c]
        for i in range(1, pc.nx):
            copy_to(ref, ref, self.sems.at[0], self.sems.at[1], pc.along_x(i)[1]).start()
        self.own().start()

    def some(self, i):
        ref = self.buf.at[pl.ds(0, self.pc.nx - 1), 0]
        return copy_to(ref, ref, self.sems.at[i], self.sems.at[i + 1], self.pc.partner())

    def relay(self):
        pc = self.pc
        self.some(0).wait_recv()
        for i in range(1, pc.nx):
            ref = self.buf.at[pc.along_x(i)[0], pc.c]
            copy_to(ref, ref, self.sems.at[4], self.sems.at[5], pc.partner()).start()

    def wait(self):
        self.own().wait_recv()
        self.some(4).wait_recv()

    def drain(self):
        self.some(0).wait_send()
        self.own().wait_send()
        self.some(4).wait_send()


def nt_dot(a, b):
    return lax.dot_general(a, b, (((1,), (1,)), ((), ())), preferred_element_type=f32)


def turned(column):
    return jnp.broadcast_to(column, (column.shape[0], 128)).T[0:1]


def column_of(row):
    return jnp.broadcast_to(row, (128, row.shape[1])).T


def body(
    nfs, nt,
    tok, mix_gain, vw, gw, taps, chan_gain, ow, mlp_gain, uw, dw,
    out,
    x, normed, gb, ob, ub, vb, db, eb,
    padded, conv, stats, hid, mo, mp, mm, mr, nm, resid, aq, ap,
    fx, fp, fm, fr, og,
    load_sem, out_sem, sems, st_sem, mx_sem, nm_sem, fx_sem, og_sem,
):
    pc = Place(nfs, nt)
    rows, width, tokens = nm.shape[2], x.shape[1], x.shape[0]
    seqs = tokens // LEN
    last = pc.half
    wq, uc, dc = vw.shape[1], ub.shape[2], db.shape[2]
    halves = wq // 128
    reach = taps.shape[0] // 2

    def load(src, dst, i):
        copy = pltpu.make_async_copy(src, dst, load_sem.at[i])
        copy.start()
        return copy

    own = dict(
        g=[load(vw, gb.at[pc.f, :, pl.ds(0, wq)], 0), load(gw, gb.at[pc.f, :, pl.ds(wq, wq)], 1)],
        o=[load(ow, ob.at[pc.f], 2)],
        u=[load(uw.at[:, pl.ds(0, uc)], ub.at[pc.f], 3)],
        v=[load(uw.at[:, pl.ds(uc, uw.shape[1] - uc)], vb.at[pc.f], 4)],
        d=[load(dw.at[:, pl.ds(0, dc)], db.at[pc.f], 5)],
        e=[load(dw.at[:, pl.ds(dc, dw.shape[1] - dc)], eb.at[pc.f], 6)],
    )
    tok_load = load(tok, x, 7)

    barrier = pltpu.get_barrier_semaphore()
    friends = [pc.dev(dz, 0) for dz in (1, -1, 2, -2)] + [pc.dev(0, dy) for dy in (1, -1, 2)]
    friends += [(pc.f, lax.rem(pc.t + i, nt)) for i in range(1, nt)]
    for dev in friends:
        pl.semaphore_signal(barrier, inc=1, device_id=dev, device_id_type=MESH)
    own["g"][0].wait()
    own["g"].pop(0)
    pl.semaphore_wait(barrier, len(friends))

    stream = {
        name: kind(pc, w, sems[i], own[name], stride)
        for i, (name, kind, w, stride) in enumerate((
            ("g", ZFirst, gb, 2), ("o", ZFirst, ob, 2), ("u", ZFirst, ub, 1), ("v", YFirst, vb, 1),
            ("d", ZFirst, db, 1), ("e", YFirst, eb, 1),
        ))
    }
    mix_sum = PairSum(pc, mo.at[1 - pc.c], mp, mm, mr, mx_sem)
    norm_all = PairGather(pc, nm, nm_sem)
    feed_sum = [
        PairSum(pc, fx[g].at[1 - pc.c], fp[g], fm[g], fr[g], fx_sem.at[g]) for g in range(len(GROUPS))
    ]
    feed_all = [PairGather(pc, og[g], og_sem.at[g]) for g in range(len(GROUPS))]

    def stat_copy(i):
        to = lax.rem(pc.t + i, nt)
        return copy_to(stats.at[pc.t], stats.at[pc.t], st_sem.at[0], st_sem.at[1], (pc.f, to))

    def stat_all():
        some = stats.at[pl.ds(0, nt - 1)]
        return copy_to(some, some, st_sem.at[0], st_sem.at[1], pc.partner())

    def norm_in():
        tok_load.wait()

        def some_rows(i, carry):
            at = pl.ds(pl.multiple_of(i * 32, 32), 32)
            s = x[at].astype(f32)
            scale = lax.rsqrt(jnp.mean(s * s, axis=-1, keepdims=True) + FLOOR)
            normed[at] = (s * scale * mix_gain[...]).astype(bf16)
            return carry

        lax.fori_loop(0, tokens // 32, some_rows, 0)

    def glu():
        for k in range(last + 1):
            stream["g"].all_of(k)
        n_all = normed[...]
        values = jnp.dot(n_all, gb[:, :, pl.ds(0, wq)].reshape(width, wq), preferred_element_type=f32)
        gating = jnp.dot(n_all, gb[:, :, pl.ds(wq, wq)].reshape(width, wq), preferred_element_type=f32)
        glued = (values * jax.nn.sigmoid(gating)).astype(bf16).astype(f32)
        zeros = jnp.zeros((16, 128), f32)
        for h in range(halves):
            for s in range(seqs):
                padded[h, s, pl.ds(0, 16)] = zeros
                padded[h, s, pl.ds(16, LEN)] = glued[s * LEN : (s + 1) * LEN, h * 128 : (h + 1) * 128]
                padded[h, s, pl.ds(16 + LEN, 16)] = zeros

    def convolve():
        for h in range(halves):
            for s in range(seqs):
                total = jnp.zeros((LEN, 128), f32)
                for o in range(taps.shape[0]):
                    tap = taps[pl.ds(o, 1), pl.ds(h * 128, 128)]
                    total = total + padded[h, s, pl.ds(16 - reach + o, LEN)] * tap
                conv[h, pl.ds(s * LEN, LEN)] = total
        sums = sum(jnp.sum(conv[h], axis=-1, keepdims=True) for h in range(halves))
        squares = sum(jnp.sum(conv[h] * conv[h], axis=-1, keepdims=True) for h in range(halves))
        stats[pc.t, pl.ds(0, 1)] = turned(sums)
        stats[pc.t, pl.ds(1, 1)] = turned(squares)
        for i in range(1, nt):
            stat_copy(i).start()

    def mix_rows(core):
        left = hid[:, core].reshape(tokens // 2, wq)
        for c in range(width // 256):
            w = ob[pl.ds(c * 8, 8)].reshape(256, wq)
            mo[core, :, :, pl.ds(c * 256, 256)] = nt_dot(left, w).astype(bf16).reshape(pc.nx, rows, 256)

    def channel_norm():
        stat_all().wait_recv()
        all_stats = jnp.sum(stats[...], axis=0)
        channels = wq * nt
        centre = column_of(all_stats[0:1]) / channels
        spread = column_of(all_stats[1:2]) / channels - centre * centre
        scale = lax.rsqrt(spread + FLOOR)
        for h in range(halves):
            at = pl.ds(h * 128, 128)
            v = (conv[h] - centre) * scale * chan_gain[:, at]
            hid[:, :, :, at] = (v * jax.nn.sigmoid(v)).astype(bf16).reshape(pc.nx, 2, rows, 128)
        for k in range(last + 1):
            stream["o"].all_of(k)
        mix_rows(1 - pc.c)
        mix_sum.swap().start()

    def mix_pair():
        mix_sum.swap().wait_recv()
        for i in range(pc.nx):
            mm[i] = (mo[pc.c, i].astype(f32) + mp[i].astype(f32)).astype(bf16)
        mix_sum.spread()

    def norm_mid():
        mix_sum.three().wait_recv()
        mr[pc.x] = mm[pc.x]
        mixed = sum(mr[i].astype(f32) for i in range(pc.nx))
        mine = x[pl.ds(pl.multiple_of(pc.t * rows, rows), rows)].astype(f32)
        res = mine + mixed.astype(bf16).astype(f32)
        resid[...] = res
        scale = lax.rsqrt(jnp.mean(res * res, axis=-1, keepdims=True) + FLOOR)
        nm[pc.x, pc.c] = (res * scale * mlp_gain[...]).astype(bf16)
        norm_all.start()

    def up():
        norm_all.wait()
        for k in range(last + 1):
            stream["u"].all_of(k)
            stream["v"].all_of(k)
        n_mlp = nm[...].reshape(tokens, width)
        for src, dst in ((ub, aq), (vb, ap)):
            cols = src.shape[2]
            for c in range(0, cols, 256):
                n = min(256, cols - c)
                a = jnp.dot(n_mlp, src[:, :, pl.ds(c, n)].reshape(width, n), preferred_element_type=f32)
                a = jnp.maximum(a, 0.0)
                dst[:, pl.ds(c, n)] = (a * a).astype(bf16)

    def slots(g):
        return [dz for k in GROUPS[g] for dz in pc.shifts(k)]

    def down(g):
        for k in GROUPS[g]:
            stream["d"].all_of(k)
            stream["e"].all_of(k)
        left = jnp.concatenate([aq[...], ap[...]], axis=1)
        for s, dz in enumerate(slots(g)):
            b = pl.ds(pc.row(dz) * NY, NY)
            part = nt_dot(left[:, :dc], db[b].reshape(128, dc))
            part = part + nt_dot(left[:, dc:], eb[b].reshape(128, eb.shape[2]))
            part = part.astype(bf16).reshape(pc.nx, 2, rows, 128)
            for core in range(2):
                fx[g][core, :, :, pl.ds(s * 128, 128)] = part[:, core]
        feed_sum[g].swap().start()

    def feed_pair(g):
        feed_sum[g].swap().wait_recv()
        for i in range(pc.nx):
            fm[g][i] = (fx[g][pc.c, i].astype(f32) + fp[g][i].astype(f32)).astype(bf16)
        feed_sum[g].spread()

    def finish(g):
        feed_sum[g].three().wait_recv()
        fr[g][pc.x] = fm[g][pc.x]
        for s, dz in enumerate(slots(g)):
            at = pl.ds(s * 128, 128)
            feed = sum(fr[g][i, :, at].astype(f32) for i in range(pc.nx))
            to = pl.ds(pl.multiple_of(pc.row(dz) * 128, 128), 128)
            og[g][pc.x, pc.c, :, at] = (resid[:, to] + feed.astype(bf16).astype(f32)).astype(bf16)
        feed_all[g].start()

    def write(g):
        feed_all[g].wait()
        for s, dz in enumerate(slots(g)):
            to = pl.ds(pl.multiple_of(pc.row(dz) * 128, 128), 128)
            pltpu.make_async_copy(og[g].at[:, :, :, pl.ds(s * 128, 128)], out.at[:, :, :, to], out_sem).start()

    steps = dict(
        N=norm_in, G=glu, C=convolve, H=channel_norm, I=lambda: mix_rows(pc.c), B=mix_pair, E=norm_mid,
        L=norm_all.relay, U=up,
    )
    by_group = dict(M=down, S=feed_pair, F=finish, R=lambda g: feed_all[g].relay(), W=write)
    for name in ORDER:
        if "." in name:
            getattr(stream[name[0]], name[2])(int(name[3:]))
        elif name in steps:
            steps[name]()
        else:
            by_group[name[0]](int(name[1:]))

    for s in stream.values():
        s.drain()
    stat_all().wait_send()
    for s in [mix_sum, *feed_sum]:
        s.swap().wait_send()
        s.three().wait_send()
    for s in [norm_all, *feed_all]:
        s.drain()
    pltpu.make_async_copy(out, out, out_sem).wait()


def layer(nfs, nt, tok, mix_gain, vw, gw, taps, chan_gain, ow, mlp_gain, uw, dw):
    tokens, width = tok.shape
    k_rows, wq = vw.shape
    ff = uw.shape[1]
    rows, nx = tokens // nt, nt // 2
    last = nfs // NY // 2
    uc, dc = ff * 5 // 8, ff // 2
    dma = pltpu.SemaphoreType.DMA
    z_first = lambda: [dma(()), dma((2, last + 1)), dma((2, last + 1)), dma((2, last + 1))]
    y_first = lambda: [dma(()), dma((2, last + 1, 2)), dma((2, 1)), dma((2, 1))]
    widths = [sum(1 if k in (0, last) else 2 for k in g) * 128 for g in GROUPS]
    block = lambda c: pltpu.VMEM((nfs, k_rows, c), bf16)
    pairs = lambda w: pltpu.VMEM((2, nx, rows, w), bf16)
    four = lambda w: pltpu.VMEM((nx, rows, w), bf16)
    eight = lambda w: pltpu.VMEM((nx, 2, rows, w), bf16)
    hbm, vmem = pl.BlockSpec(memory_space=pl.ANY), pl.BlockSpec(memory_space=pltpu.VMEM)
    scratch = [
        pltpu.VMEM((tokens, width), bf16),
        pltpu.VMEM((tokens, width), bf16),
        block(2 * wq), block(wq), block(uc), block(ff - uc), block(dc), block(ff - dc),
        pltpu.VMEM((wq // 128, tokens // LEN, LEN + 32, 128), f32),
        pltpu.VMEM((wq // 128, tokens, 128), f32),
        pltpu.VMEM((nt, 2, tokens), f32),
        eight(wq),
        pairs(width), four(width), four(width), four(width),
        eight(width),
        pltpu.VMEM((rows, width), f32),
        pltpu.VMEM((tokens, uc), bf16),
        pltpu.VMEM((tokens, ff - uc), bf16),
        [pairs(w) for w in widths], [four(w) for w in widths], [four(w) for w in widths],
        [four(w) for w in widths], [eight(w) for w in widths],
        dma((8,)), dma(()),
        [z_first(), z_first(), z_first(), y_first(), z_first(), y_first()],
        dma((2,)), dma((4,)), dma((6,)), dma((len(GROUPS), 4)), dma((len(GROUPS), 6)),
    ]
    done = pl.pallas_call(
        functools.partial(body, nfs, nt),
        out_shape=jax.ShapeDtypeStruct((nx, 2, rows, width), bf16),
        in_specs=[hbm, vmem, hbm, hbm, vmem, vmem, hbm, vmem, hbm, hbm],
        out_specs=hbm,
        scratch_shapes=scratch,
        compiler_params=pltpu.CompilerParams(
            collective_id=0, has_side_effects=True, vmem_limit_bytes=56 * 1024 * 1024
        ),
        name="layer",
    )(
        tok, mix_gain.reshape(1, -1), vw, gw, taps, chan_gain.reshape(1, -1), ow.T,
        mlp_gain.reshape(1, -1), uw, dw.T,
    )
    return done.reshape(tokens, width)


def solution(mesh):
    in_specs = (
        P("fs", None), P(), P("fs", "tp"), P("fs", "tp"), P(None, "tp"),
        P("tp"), P("tp", "fs"), P(), P("fs", "tp"), P("tp", "fs"),
    )
    nfs, nt = mesh.shape["fs"], mesh.shape["tp"]
    return jax.shard_map(
        functools.partial(layer, nfs, nt), mesh=mesh, in_specs=in_specs,
        out_specs=P("fs", None), check_vma=False,
    )
```

```python
import functools

import jax
import jax.numpy as jnp
from jax import lax
from jax.experimental import pallas as pl
from jax.experimental.pallas import tpu as pltpu
from jax.sharding import PartitionSpec as P

MESH = pl.DeviceIdType.MESH
LEN = 128
NY = 4
FLOOR = 0.05
f32, bf16 = jnp.float32, jnp.bfloat16

ORDER = (
    "o.y0", "o.z0", "e.y0", "g.z0", "g.y0", "u.y0", "d.y0", "u.z0", "o.y1", "o.z1", "g.z1", "v.y0", "g.y1", "g.z2",
    "g.y2", "g.f0", "o.z2", "v.y1", "u.z1", "o.y2", "g.z3", "g.y3", "N", "g.f1", "o.z3", "g.z4", "v.z00", "g.f2",
    "g.y4", "o.y3", "g.z5", "g.y5", "o.z4", "g.f3", "g.z6", "u.z2", "e.y1", "g.y6", "v.z01", "g.y7", "d.z0", "o.z5",
    "v.z10", "g.y8", "g.f4", "u.z3", "g.f5", "v.z11", "g.f6", "o.z6", "e.z00", "g.f7", "g.f8", "d.z1", "o.y5", "o.f0",
    "o.y6", "o.y4", "o.f2", "v.z20", "o.y7", "u.y3", "o.z7", "e.z01", "G", "v.z21", "o.f5", "u.z4", "o.y8", "d.z2",
    "u.y2", "e.z10", "o.f7", "o.f6", "v.z30", "o.f1", "C", "o.f3", "o.f4", "o.f8", "u.f3", "u.y5", "u.z5", "v.z31",
    "u.y1", "u.y4", "d.z3", "e.z11", "v.z40", "H", "u.y6", "v.z41", "I", "u.f2", "u.z6", "B0", "u.f5", "e.z21",
    "v.z50", "B1", "v.z51", "u.y7", "e.z20", "u.z7", "u.f4", "E0", "u.f6", "u.f0", "d.z4", "d.y2", "v.z60", "v.z61",
    "E1", "e.z30", "u.y8", "d.z5", "d.y1", "u.f1", "e.z31", "v.z70", "L0", "u.f7", "u.f8", "v.z71", "d.f0", "d.f2",
    "L1", "d.f1", "d.y4", "e.z40", "e.z41", "d.y3", "d.z6", "d.y6", "d.y5", "U", "e.z50", "M0", "d.f4", "e.z51",
    "d.f3", "S0", "d.y7", "d.z7", "d.f6", "e.z60", "d.f5", "e.z61", "M1", "F0", "d.f7", "d.y8", "S1", "e.z70", "M2",
    "e.z71", "S2", "M3", "S3", "M4", "F1", "F2", "R0", "F3", "F4", "W0", "R1", "R2", "W1", "R3", "W2", "W4", "W3",
)
GROUPS = ((0, 1, 2), (3, 4), (5, 6), (7,), (8,))
STRIDE = {'g': 2}
DIRECT = {'d': 8}
PARTS = 2


def copy_to(src, dst, ssem, rsem, dev):
    return pltpu.make_async_remote_copy(
        src_ref=src, dst_ref=dst, send_sem=ssem, recv_sem=rsem, device_id=dev, device_id_type=MESH
    )


class Place:
    def __init__(self, nfs, nt):
        self.f, self.t = lax.axis_index("fs"), lax.axis_index("tp")
        self.nz = nfs // NY
        self.half = self.nz // 2
        self.z, self.y = self.f // NY, lax.rem(self.f, NY)
        self.nx = nt // 2
        self.x, self.c = self.t // 2, lax.rem(self.t, 2)

    def row(self, dz):
        return lax.rem(self.z + (dz + self.nz), self.nz)

    def blk(self, dz, dy):
        return self.row(dz) * NY + lax.rem(self.y + (dy + NY), NY)

    def dev(self, dz, dy):
        return (self.blk(dz, dy), self.t)

    def along_x(self, i):
        x = lax.rem(self.x + i, self.nx)
        return x, (self.f, x * 2 + self.c)

    def partner(self):
        return (self.f, self.x * 2 + 1 - self.c)

    def shifts(self, k):
        if k == 0:
            return (0,)
        return (self.half,) if k == self.half else (-k, k)


class Stream:
    def __init__(self, pc, w, sems, loads, stride, direct):
        self.pc, self.w, self.loads, self.stride, self.direct = pc, w, loads, stride, direct
        self.ss, self.zr, self.yr, self.hr = sems
        self.n = w.shape[1] // 2
        self.came = set()

    def part(self, b, which):
        return self.w.at[b, pl.ds(which * self.n, self.n)]

    def send(self, ref, rsem, dev):
        copy_to(ref, ref, self.ss, rsem, dev).start()

    def await_(self, ref, rsem):
        copy_to(ref, ref, self.ss, rsem, self.pc.dev(1, 0)).wait_recv()

    def need(self, *key):
        if key not in self.came:
            self.came.add(key)
            self.arrive(*key)

    def own(self):
        if "own" not in self.came:
            self.came.add("own")
            for load in self.loads:
                load.wait()

    def drain(self):
        whole = self.w.at[pl.ds(0, self.w.shape[0] - 1)]
        copy_to(whole, whole, self.ss, self.yr.at[0, 0], self.pc.dev(1, 0)).wait_send()


class ZFirst(Stream):
    def arrive(self, what, k):
        pc = self.pc
        for d in range(2):
            if what == "z":
                b = pc.blk(k if d else -k, 0)
                self.await_(self.part(b, d) if k == pc.half else self.w.at[b], self.zr.at[d, k])
            elif what == "y":
                self.await_(self.w.at[pl.ds(0, len(pc.shifts(k)))], self.yr.at[d, k])
            elif k >= self.direct:
                if d == 0:
                    self.await_(self.w.at[pl.ds(0, len(pc.shifts(k)))], self.hr.at[0, k])
            else:
                self.await_(self.w.at[0] if len(pc.shifts(k)) == 2 else self.part(0, d), self.hr.at[d, k])

    def all_of(self, k):
        self.own()
        for what in "zyh" if k else "yh":
            self.need(what, k)

    def ready(self, k):
        if k:
            self.need("z", k)
        else:
            self.own()

    def z(self, k):
        pc = self.pc
        self.ready(k)
        for step in range(1, self.stride + 1) if k == 0 else (self.stride,):
            for d, way in ((0, 1), (1, -1)):
                b = pc.blk(-way * k, 0)
                ref = self.part(b, d) if k + step == pc.half else self.w.at[b]
                self.send(ref, self.zr.at[d, k + step], pc.dev(way * step, 0))

    def y(self, k):
        pc = self.pc
        self.ready(k)
        for dz in pc.shifts(k):
            ref = self.w.at[pc.blk(dz, 0)]
            for d, way in ((0, 1), (1, -1)):
                self.send(ref, self.yr.at[d, k], pc.dev(0, way))
            if k >= self.direct:
                self.send(ref, self.hr.at[0, k], pc.dev(0, 2))

    def f(self, k):
        pc = self.pc
        self.need("y", k)
        for dz in pc.shifts(k):
            for d, way in ((0, 1), (1, -1)):
                self.send(self.part(pc.blk(dz, -way), d), self.hr.at[d, k], pc.dev(0, way))


class YFirst(Stream):
    def two(self, dz, h):
        return self.w.at[pl.ds(self.pc.row(dz) * NY + h * 2, 2)]

    def arrive(self, what, k, h=0):
        pc = self.pc
        for d, way in ((0, 1), (1, -1)):
            if what == "y":
                self.await_(self.w.at[pc.blk(0, -way)], self.yr.at[d, 0])
            elif what == "h":
                self.await_(self.part(pc.blk(0, 2), d), self.hr.at[d, 0])
            elif k < pc.half or d == h:
                self.await_(self.two(-way * k, h), self.zr.at[d, k, h])

    def all_of(self, k):
        self.own()
        if k:
            for h in range(2):
                self.need("z", k, h)
        else:
            self.need("y", 0)
            self.need("h", 0)

    def y(self, k):
        pc = self.pc
        if k == 0:
            self.own()
        else:
            self.need("y", 0)
        for d, way in ((0, 1), (1, -1)):
            if k == 0:
                self.send(self.w.at[pc.f], self.yr.at[d, 0], pc.dev(0, way))
            else:
                self.send(self.part(pc.blk(0, -way), d), self.hr.at[d, 0], pc.dev(0, way))

    def z(self, kh):
        pc = self.pc
        k, h = kh // 10, kh % 10
        if k:
            self.need("z", k, h)
        else:
            self.all_of(0)
        for d, way in ((0, 1), (1, -1)):
            if k + 1 < pc.half or d == h:
                self.send(self.two(-way * k, h), self.zr.at[d, k + 1, h], pc.dev(way, 0))


class PairSum:
    def __init__(self, pc, other, got, mine, came, sems):
        self.pc, self.other, self.got, self.mine, self.came, self.sems = pc, other, got, mine, came, sems

    def swap(self):
        return copy_to(self.other, self.got, self.sems.at[0], self.sems.at[1], self.pc.partner())

    def spread(self):
        pc = self.pc
        for i in range(1, pc.nx):
            x, dev = pc.along_x(i)
            copy_to(self.mine.at[x], self.came.at[pc.x], self.sems.at[2], self.sems.at[3], dev).start()

    def three(self):
        some = self.came.at[pl.ds(0, self.pc.nx - 1)]
        return copy_to(some, some, self.sems.at[2], self.sems.at[3], self.pc.partner())


class PairGather:
    def __init__(self, pc, buf, sems):
        self.pc, self.buf, self.sems = pc, buf, sems

    def own(self):
        pc = self.pc
        ref = self.buf.at[pc.t]
        return copy_to(ref, ref, self.sems.at[2], self.sems.at[3], pc.partner())

    def start(self):
        pc = self.pc
        ref = self.buf.at[pc.t]
        for i in range(1, pc.nx):
            copy_to(ref, ref, self.sems.at[0], self.sems.at[1], pc.along_x(i)[1]).start()
        self.own().start()

    def some(self, i):
        ref = self.buf.at[pl.ds(0, self.pc.nx - 1)]
        return copy_to(ref, ref, self.sems.at[i], self.sems.at[i + 1], self.pc.partner())

    def relay(self):
        pc = self.pc
        self.some(0).wait_recv()
        for i in range(1, pc.nx):
            ref = self.buf.at[pc.along_x(i)[0] * 2 + pc.c]
            copy_to(ref, ref, self.sems.at[4], self.sems.at[5], pc.partner()).start()

    def wait(self):
        self.own().wait_recv()
        self.some(4).wait_recv()

    def drain(self):
        self.some(0).wait_send()
        self.own().wait_send()
        self.some(4).wait_send()


class Exchange:
    def __init__(self, pc, piece, came, sems):
        self.pc, self.piece, self.came, self.sems = pc, piece, came, sems

    def start(self):
        pc, nt = self.pc, self.pc.nx * 2
        for i in range(1, nt):
            to = lax.rem(pc.t + i, nt)
            dst = self.came.at[pc.t]
            copy_to(self.piece(to), dst, self.sems.at[0], self.sems.at[1], (pc.f, to)).start()

    def rest(self):
        some = self.came.at[pl.ds(0, self.pc.nx * 2 - 1)]
        return copy_to(some, some, self.sems.at[0], self.sems.at[1], self.pc.partner())


def nt_dot(a, b):
    return lax.dot_general(a, b, (((1,), (1,)), ((), ())), preferred_element_type=f32)


def turned(column):
    return jnp.broadcast_to(column, (column.shape[0], 128)).T[0:1]


def column_of(row):
    return jnp.broadcast_to(row, (128, row.shape[1])).T


def body(
    nfs, nt,
    tok, mix_gain_in, vw, gw, taps_in, chan_gain_in, ow, mlp_gain_in, uw, dw,
    out,
    mix_gain, taps, chan_gain, mlp_gain,
    x, normed, gb, ob, ub, vb, db, eb,
    padded, conv, stats, hid, mo, mp, mm, mr, nm, resid, aq, ap,
    fx, fp, fm, fr, og,
    load_sem, sems, st_sem, mx_sem, nm_sem, fx_sem, og_sem,
):
    pc = Place(nfs, nt)
    rows, width, tokens = nm.shape[1], x.shape[1], x.shape[0]
    seqs = tokens // LEN
    last = pc.half
    wq, uc, dc = vw.shape[1], ub.shape[2], db.shape[2]
    halves = wq // 128
    reach = taps.shape[0] // 2

    def load(src, dst, i):
        copy = pltpu.make_async_copy(src, dst, load_sem.at[i])
        copy.start()
        return copy

    own = dict(
        g=[load(vw, gb.at[pc.f, :, pl.ds(0, wq)], 0), load(gw, gb.at[pc.f, :, pl.ds(wq, wq)], 1)],
        o=[load(ow, ob.at[pc.f], 2)],
        u=[load(uw.at[:, pl.ds(0, uc)], ub.at[pc.f], 3)],
        v=[load(uw.at[:, pl.ds(uc, uw.shape[1] - uc)], vb.at[pc.f], 4)],
        d=[load(dw.at[:, pl.ds(0, dc)], db.at[pc.f], 5)],
        e=[load(dw.at[:, pl.ds(dc, dw.shape[1] - dc)], eb.at[pc.f], 6)],
    )
    tok_load = load(tok, x, 7)
    small = [
        load(src, dst, 8 + i)
        for i, (src, dst) in enumerate((
            (mix_gain_in, mix_gain), (taps_in, taps), (chan_gain_in, chan_gain), (mlp_gain_in, mlp_gain),
        ))
    ]

    barrier = pltpu.get_barrier_semaphore()
    friends = [pc.dev(dz, 0) for dz in (1, -1, 2, -2)] + [pc.dev(0, dy) for dy in (1, -1, 2)]
    friends += [(pc.f, lax.rem(pc.t + i, nt)) for i in range(1, nt)]
    for dev in friends:
        pl.semaphore_signal(barrier, inc=1, device_id=dev, device_id_type=MESH)
    own["g"][0].wait()
    own["g"].pop(0)
    pl.semaphore_wait(barrier, len(friends))

    stream = {
        name: kind(pc, w, sems[i], own[name], STRIDE.get(name, 1), DIRECT.get(name, last + 1))
        for i, (name, kind, w) in enumerate((
            ("g", ZFirst, gb), ("o", ZFirst, ob), ("u", ZFirst, ub), ("v", YFirst, vb), ("d", ZFirst, db),
            ("e", YFirst, eb),
        ))
    }
    part_rows = rows // PARTS
    parts = [pl.ds(i * part_rows, part_rows) for i in range(PARTS)]
    mix_sum = [
        PairSum(pc, mo.at[1 - pc.c, :, p], mp.at[:, p], mm.at[:, p], mr.at[:, p], mx_sem.at[i])
        for i, p in enumerate(parts)
    ]
    norm_all = [PairGather(pc, nm.at[:, p], nm_sem.at[i]) for i, p in enumerate(parts)]
    end = len(GROUPS) - 1
    feed_sum = [PairSum(pc, fx[g].at[1 - pc.c], fp[g], fm[g], fr[g], fx_sem.at[g]) for g in range(end)]
    feed_all = [PairGather(pc, og[g], og_sem.at[g]) for g in range(end)]
    end_sum = Exchange(pc, lambda to: fx[end].at[lax.rem(to, 2), to // 2], fr[end], fx_sem.at[end])
    end_all = Exchange(pc, lambda to: og[end].at[pc.t], og[end], og_sem.at[end])
    stat_all = Exchange(pc, lambda to: stats.at[pc.t], stats, st_sem)

    def norm_in():
        for copy in (tok_load, *small):
            copy.wait()

        def some_rows(i, carry):
            at = pl.ds(pl.multiple_of(i * 32, 32), 32)
            s = x[at].astype(f32)
            scale = lax.rsqrt(jnp.mean(s * s, axis=-1, keepdims=True) + FLOOR)
            normed[at] = (s * scale * mix_gain[...]).astype(bf16)
            return carry

        lax.fori_loop(0, tokens // 32, some_rows, 0)

    def glu():
        for k in range(last + 1):
            stream["g"].all_of(k)
        n_all = normed[...]
        values = jnp.dot(n_all, gb[:, :, pl.ds(0, wq)].reshape(width, wq), preferred_element_type=f32)
        gating = jnp.dot(n_all, gb[:, :, pl.ds(wq, wq)].reshape(width, wq), preferred_element_type=f32)
        glued = (values * jax.nn.sigmoid(gating)).astype(bf16).astype(f32)
        zeros = jnp.zeros((16, 128), f32)
        for h in range(halves):
            for s in range(seqs):
                padded[h, s, pl.ds(0, 16)] = zeros
                padded[h, s, pl.ds(16, LEN)] = glued[s * LEN : (s + 1) * LEN, h * 128 : (h + 1) * 128]
                padded[h, s, pl.ds(16 + LEN, 16)] = zeros

    def convolve():
        for h in range(halves):
            for s in range(seqs):
                total = jnp.zeros((LEN, 128), f32)
                for o in range(taps.shape[0]):
                    tap = taps[pl.ds(o, 1), pl.ds(h * 128, 128)]
                    total = total + padded[h, s, pl.ds(16 - reach + o, LEN)] * tap
                conv[h, pl.ds(s * LEN, LEN)] = total
        sums = sum(jnp.sum(conv[h], axis=-1, keepdims=True) for h in range(halves))
        squares = sum(jnp.sum(conv[h] * conv[h], axis=-1, keepdims=True) for h in range(halves))
        stats[pc.t, pl.ds(0, 1)] = turned(sums)
        stats[pc.t, pl.ds(1, 1)] = turned(squares)
        stat_all.start()

    def mix_rows(core):
        left = hid[:, core].reshape(tokens // 2, wq)
        for c in range(width // 256):
            w = ob[pl.ds(c * 8, 8)].reshape(256, wq)
            mo[core, :, :, pl.ds(c * 256, 256)] = nt_dot(left, w).astype(bf16).reshape(pc.nx, rows, 256)

    def channel_norm():
        stat_all.rest().wait_recv()
        all_stats = jnp.sum(stats[...], axis=0)
        channels = wq * nt
        centre = column_of(all_stats[0:1]) / channels
        spread = column_of(all_stats[1:2]) / channels - centre * centre
        scale = lax.rsqrt(spread + FLOOR)
        for h in range(halves):
            at = pl.ds(h * 128, 128)
            v = (conv[h] - centre) * scale * chan_gain[:, at]
            hid[:, :, :, at] = (v * jax.nn.sigmoid(v)).astype(bf16).reshape(pc.nx, 2, rows, 128)
        for k in range(last + 1):
            stream["o"].all_of(k)
        mix_rows(1 - pc.c)
        for m in mix_sum:
            m.swap().start()

    def mix_pair(i):
        p = parts[i]
        mix_sum[i].swap().wait_recv()
        for j in range(pc.nx):
            mm[j, p] = (mo[pc.c, j, p].astype(f32) + mp[j, p].astype(f32)).astype(bf16)
        mix_sum[i].spread()

    def norm_mid(i):
        p = parts[i]
        mix_sum[i].three().wait_recv()
        mr[pc.x, p] = mm[pc.x, p]
        mixed = sum(mr[j, p].astype(f32) for j in range(pc.nx))
        at = pl.multiple_of(pc.t * rows + i * part_rows, part_rows)
        res = x[pl.ds(at, part_rows)].astype(f32) + mixed.astype(bf16).astype(f32)
        resid[p] = res
        scale = lax.rsqrt(jnp.mean(res * res, axis=-1, keepdims=True) + FLOOR)
        nm[pc.t, p] = (res * scale * mlp_gain[...]).astype(bf16)
        norm_all[i].start()

    def up():
        for n in norm_all:
            n.wait()
        for k in range(last + 1):
            stream["u"].all_of(k)
            stream["v"].all_of(k)
        n_mlp = nm[...].reshape(tokens, width)
        for src, dst in ((ub, aq), (vb, ap)):
            cols = src.shape[2]
            for c in range(0, cols, 256):
                n = min(256, cols - c)
                a = jnp.dot(n_mlp, src[:, :, pl.ds(c, n)].reshape(width, n), preferred_element_type=f32)
                a = jnp.maximum(a, 0.0)
                dst[:, pl.ds(c, n)] = (a * a).astype(bf16)

    def slots(g):
        return [dz for k in GROUPS[g] for dz in pc.shifts(k)]

    def down(g):
        for k in GROUPS[g]:
            stream["d"].all_of(k)
            stream["e"].all_of(k)
        left = jnp.concatenate([aq[...], ap[...]], axis=1)
        for s, dz in enumerate(slots(g)):
            b = pl.ds(pc.row(dz) * NY, NY)
            part = nt_dot(left[:, :dc], db[b].reshape(128, dc))
            part = part + nt_dot(left[:, dc:], eb[b].reshape(128, eb.shape[2]))
            part = part.astype(bf16).reshape(pc.nx, 2, rows, 128)
            for core in range(2):
                fx[g][core, :, :, pl.ds(s * 128, 128)] = part[:, core]
        if g == end:
            end_sum.start()
        else:
            feed_sum[g].swap().start()

    def feed_pair(g):
        feed_sum[g].swap().wait_recv()
        for i in range(pc.nx):
            fm[g][i] = (fx[g][pc.c, i].astype(f32) + fp[g][i].astype(f32)).astype(bf16)
        feed_sum[g].spread()

    def finish(g):
        if g == end:
            end_sum.rest().wait_recv()
            fr[g][pc.t] = fx[g][pc.c, pc.x]
        else:
            feed_sum[g].three().wait_recv()
            fr[g][pc.x] = fm[g][pc.x]
        for s, dz in enumerate(slots(g)):
            at = pl.ds(s * 128, 128)
            feed = sum(fr[g][i, :, at].astype(f32) for i in range(fr[g].shape[0]))
            to = pl.ds(pl.multiple_of(pc.row(dz) * 128, 128), 128)
            og[g][pc.t, :, at] = (resid[:, to] + feed.astype(bf16).astype(f32)).astype(bf16)
        if g == end:
            end_all.start()
        else:
            feed_all[g].start()

    def write(g):
        if g == end:
            end_all.rest().wait_recv()
        else:
            feed_all[g].wait()
        for s, dz in enumerate(slots(g)):
            to = pl.ds(pl.multiple_of(pc.row(dz) * 128, 128), 128)
            out[:, :, to] = og[g][:, :, pl.ds(s * 128, 128)]

    steps = dict(N=norm_in, G=glu, C=convolve, H=channel_norm, I=lambda: mix_rows(pc.c), U=up)
    by_number = dict(
        B=mix_pair, E=norm_mid, L=lambda i: norm_all[i].relay(),
        M=down, S=feed_pair, F=finish, R=lambda g: feed_all[g].relay(), W=write,
    )
    for name in ORDER:
        if "." in name:
            getattr(stream[name[0]], name[2])(int(name[3:]))
        elif name in steps:
            steps[name]()
        else:
            by_number[name[0]](int(name[1:]))

    for s in stream.values():
        s.drain()
    for s in [stat_all, end_sum, end_all]:
        s.rest().wait_send()
    for s in [*mix_sum, *feed_sum]:
        s.swap().wait_send()
        s.three().wait_send()
    for s in [*norm_all, *feed_all]:
        s.drain()


def layer(nfs, nt, tok, mix_gain, vw, gw, taps, chan_gain, ow, mlp_gain, uw, dw):
    tokens, width = tok.shape
    k_rows, wq = vw.shape
    ff = uw.shape[1]
    rows, nx = tokens // nt, nt // 2
    last = nfs // NY // 2
    uc, dc = ff * 5 // 8, ff // 2
    dma = pltpu.SemaphoreType.DMA
    z_first = lambda: [dma(()), dma((2, last + 1)), dma((2, last + 1)), dma((2, last + 1))]
    y_first = lambda: [dma(()), dma((2, last + 1, 2)), dma((2, 1)), dma((2, 1))]
    widths = [sum(1 if k in (0, last) else 2 for k in g) * 128 for g in GROUPS]
    block = lambda c: pltpu.VMEM((nfs, k_rows, c), bf16)
    pairs = lambda w: pltpu.VMEM((2, nx, rows, w), bf16)
    four = lambda w: pltpu.VMEM((nx, rows, w), bf16)
    eight = lambda w: pltpu.VMEM((nt, rows, w), bf16)
    hbm, vmem = pl.BlockSpec(memory_space=pltpu.HBM), pl.BlockSpec(memory_space=pltpu.VMEM)
    scratch = [
        pltpu.VMEM((1, width), f32), pltpu.VMEM(taps.shape, f32), pltpu.VMEM((1, wq), f32), pltpu.VMEM((1, width), f32),
        pltpu.VMEM((tokens, width), bf16),
        pltpu.VMEM((tokens, width), bf16),
        block(2 * wq), block(wq), block(uc), block(ff - uc), block(dc), block(ff - dc),
        pltpu.VMEM((wq // 128, tokens // LEN, LEN + 32, 128), f32),
        pltpu.VMEM((wq // 128, tokens, 128), f32),
        pltpu.VMEM((nt, 2, tokens), f32),
        pltpu.VMEM((nx, 2, rows, wq), bf16),
        pairs(width), four(width), four(width), four(width),
        eight(width),
        pltpu.VMEM((rows, width), f32),
        pltpu.VMEM((tokens, uc), bf16),
        pltpu.VMEM((tokens, ff - uc), bf16),
        [pairs(w) for w in widths], [four(w) for w in widths], [four(w) for w in widths],
        [*(four(w) for w in widths[:-1]), eight(widths[-1])], [eight(w) for w in widths],
        dma((12,)),
        [z_first(), z_first(), z_first(), y_first(), z_first(), y_first()],
        dma((2,)), dma((PARTS, 4)), dma((PARTS, 6)), dma((len(GROUPS), 4)), dma((len(GROUPS), 6)),
    ]
    done = pl.pallas_call(
        functools.partial(body, nfs, nt),
        out_shape=jax.ShapeDtypeStruct((nt, rows, width), bf16),
        in_specs=[hbm] * 10,
        out_specs=vmem,
        scratch_shapes=scratch,
        compiler_params=pltpu.CompilerParams(
            collective_id=0, has_side_effects=True, vmem_limit_bytes=40 * 1024 * 1024
        ),
        name="layer",
    )(
        *(pltpu.with_memory_space_constraint(a, pltpu.HBM) for a in (
            tok, mix_gain.reshape(1, -1), vw, gw, taps, chan_gain.reshape(1, -1), ow.T,
            mlp_gain.reshape(1, -1), uw, dw.T,
        ))
    )
    return done.reshape(tokens, width)


def solution(mesh):
    in_specs = (
        P("fs", None), P(), P("fs", "tp"), P("fs", "tp"), P(None, "tp"),
        P("tp"), P("tp", "fs"), P(), P("fs", "tp"), P("tp", "fs"),
    )
    nfs, nt = mesh.shape["fs"], mesh.shape["tp"]
    return jax.shard_map(
        functools.partial(layer, nfs, nt), mesh=mesh, in_specs=in_specs,
        out_specs=P("fs", None), check_vma=False,
    )
```

```python
import functools

import jax
import jax.numpy as jnp
from jax import lax
from jax.experimental import pallas as pl
from jax.experimental.pallas import tpu as pltpu
from jax.sharding import PartitionSpec as P

MESH = pl.DeviceIdType.MESH
LEN = 128
NY = 4
FLOOR = 0.05
f32, bf16 = jnp.float32, jnp.bfloat16

ORDER = (
    "o.z0", "o.y0", "u.z0", "e.y0", "u.y0", "d.y0", "v.y0", "g.z0", "o.z1", "d.z0", "g.y0", "e.y1", "u.y1", "u.z1",
    "g.y1", "g.z1", "v.y1", "g.y2", "o.z2", "g.z2", "o.y1", "d.z1", "u.z2", "o.y2", "o.f0", "o.z3", "u.y2", "g.y3",
    "g.z3", "g.z4", "N", "g.y4", "o.z4", "v.z00", "v.z01", "u.z3", "u.f2", "o.f1", "g.y6", "g.z5", "g.f2", "o.z5",
    "g.y5", "g.z6", "o.y3", "g.f0", "g.f4", "v.z11", "v.z10", "o.z6", "u.z4", "g.f1", "g.y7", "e.z00", "g.f5", "d.z2",
    "g.f3", "g.y8", "o.y5", "v.z21", "v.z20", "o.y7", "o.z7", "e.z10", "u.z5", "g.f6", "d.z3", "o.y4", "g.f7",
    "e.z01", "o.y8", "g.f8", "o.f3", "o.f5", "o.y6", "o.f2", "d.y1", "v.z30", "o.f7", "u.y5", "u.z6", "e.z20", "o.f8",
    "o.f4", "G", "e.z11", "v.z31", "C", "o.f6", "u.y6", "d.y4", "d.z4", "v.z40", "u.y7", "u.y4", "e.z21", "e.z30",
    "H", "u.z7", "I", "v.z41", "d.z5", "B0", "d.y2", "v.z50", "B1", "e.z31", "d.y3", "u.f3", "u.y8", "v.z51", "u.f4",
    "u.f0", "u.f7", "d.y5", "u.f6", "d.y6", "u.f1", "E0", "e.z40", "v.z60", "u.f8", "u.y3", "d.f0", "d.f3", "d.z6",
    "E1", "v.z61", "e.z41", "d.f1", "v.z70", "d.f2", "L0", "d.f5", "u.f5", "v.z71", "e.z50", "e.z51", "L1", "d.f6",
    "d.f4", "d.y7", "d.z7", "U", "e.z60", "M0", "e.z61", "M1", "M3", "d.y8", "S0", "M2", "S3", "d.f7", "S1", "S2",
    "e.z70", "e.z71", "F0", "M4", "F3", "S4", "M5", "F1", "F2", "R0", "R3", "F4", "W3", "F5", "R1", "R2", "W0", "R4",
    "W1", "W2", "W5", "W4",
)
GROUPS = ((0, 1), (2, 3), (4, 5), (6,), (7,), (8,))
STRIDE = {'g': 2}
DIRECT = {'d': 8}
VIA = {'u': (3, 5)}
PARTS = 2


def copy_to(src, dst, ssem, rsem, dev):
    return pltpu.make_async_remote_copy(
        src_ref=src, dst_ref=dst, send_sem=ssem, recv_sem=rsem, device_id=dev, device_id_type=MESH
    )


class Place:
    def __init__(self, nfs, nt):
        self.f, self.t = lax.axis_index("fs"), lax.axis_index("tp")
        self.nz = nfs // NY
        self.half = self.nz // 2
        self.z, self.y = self.f // NY, lax.rem(self.f, NY)
        self.nx = nt // 2
        self.x, self.c = self.t // 2, lax.rem(self.t, 2)

    def row(self, dz):
        return lax.rem(self.z + (dz + self.nz), self.nz)

    def blk(self, dz, dy):
        return self.row(dz) * NY + lax.rem(self.y + (dy + NY), NY)

    def dev(self, dz, dy):
        return (self.blk(dz, dy), self.t)

    def along_x(self, i):
        x = lax.rem(self.x + i, self.nx)
        return x, (self.f, x * 2 + self.c)

    def partner(self):
        return (self.f, self.x * 2 + 1 - self.c)

    def shifts(self, k):
        if k == 0:
            return (0,)
        return (self.half,) if k == self.half else (-k, k)


class Stream:
    def __init__(self, pc, w, sems, loads, stride, direct, via):
        self.pc, self.w, self.loads, self.stride, self.direct, self.via = pc, w, loads, stride, direct, via
        self.ss, self.zr, self.yr, self.hr = sems
        self.n = w.shape[1] // 2
        self.came = set()

    def part(self, b, which):
        return self.w.at[b, pl.ds(which * self.n, self.n)]

    def send(self, ref, rsem, dev):
        copy_to(ref, ref, self.ss, rsem, dev).start()

    def await_(self, ref, rsem):
        copy_to(ref, ref, self.ss, rsem, self.pc.dev(1, 0)).wait_recv()

    def need(self, *key):
        if key not in self.came:
            self.came.add(key)
            self.arrive(*key)

    def own(self):
        if "own" not in self.came:
            self.came.add("own")
            for load in self.loads:
                load.wait()

    def drain(self):
        whole = self.w.at[pl.ds(0, self.w.shape[0] - 1)]
        copy_to(whole, whole, self.ss, self.yr.at[0, 0], self.pc.dev(1, 0)).wait_send()


class ZFirst(Stream):
    def arrive(self, what, k):
        pc = self.pc
        for d in range(2):
            if what == "z":
                b = pc.blk(k if d else -k, 0)
                self.await_(self.part(b, d) if k == pc.half else self.w.at[b], self.zr.at[d, k])
            elif what == "y":
                self.await_(self.w.at[pl.ds(0, len(pc.shifts(k)))], self.yr.at[d, k])
            elif k in self.via:
                self.await_(self.w.at[pc.blk(k if d else -k, 2)], self.hr.at[d, k])
            elif k >= self.direct:
                if d == 0:
                    self.await_(self.w.at[pl.ds(0, len(pc.shifts(k)))], self.hr.at[0, k])
            else:
                self.await_(self.w.at[0] if len(pc.shifts(k)) == 2 else self.part(0, d), self.hr.at[d, k])

    def all_of(self, k):
        self.own()
        for what in "zyh" if k else "yh":
            self.need(what, k)

    def ready(self, k):
        if k:
            self.need("z", k)
        else:
            self.own()

    def z(self, k):
        pc = self.pc
        self.ready(k)
        for step in range(1, self.stride + 1) if k == 0 else (self.stride,):
            for d, way in ((0, 1), (1, -1)):
                b = pc.blk(-way * k, 0)
                ref = self.part(b, d) if k + step == pc.half else self.w.at[b]
                self.send(ref, self.zr.at[d, k + step], pc.dev(way * step, 0))

    def y(self, k):
        pc = self.pc
        self.ready(k)
        for dz in pc.shifts(k):
            ref = self.w.at[pc.blk(dz, 0)]
            for d, way in ((0, 1), (1, -1)):
                self.send(ref, self.yr.at[d, k], pc.dev(0, way))
            if k >= self.direct:
                self.send(ref, self.hr.at[0, k], pc.dev(0, 2))

    def f(self, k):
        pc = self.pc
        if k in self.via:
            self.need("h", k - 1)
            for d, way in ((0, 1), (1, -1)):
                self.send(self.w.at[pc.blk(-way * (k - 1), 2)], self.hr.at[d, k], pc.dev(way, 0))
            return
        self.need("y", k)
        for dz in pc.shifts(k):
            for d, way in ((0, 1), (1, -1)):
                self.send(self.part(pc.blk(dz, -way), d), self.hr.at[d, k], pc.dev(0, way))


class YFirst(Stream):
    def two(self, dz, h):
        return self.w.at[pl.ds(self.pc.row(dz) * NY + h * 2, 2)]

    def arrive(self, what, k, h=0):
        pc = self.pc
        for d, way in ((0, 1), (1, -1)):
            if what == "y":
                self.await_(self.w.at[pc.blk(0, -way)], self.yr.at[d, 0])
            elif what == "h":
                self.await_(self.part(pc.blk(0, 2), d), self.hr.at[d, 0])
            elif k < pc.half or d == h:
                self.await_(self.two(-way * k, h), self.zr.at[d, k, h])

    def all_of(self, k):
        self.own()
        if k:
            for h in range(2):
                self.need("z", k, h)
        else:
            self.need("y", 0)
            self.need("h", 0)

    def y(self, k):
        pc = self.pc
        if k == 0:
            self.own()
        else:
            self.need("y", 0)
        for d, way in ((0, 1), (1, -1)):
            if k == 0:
                self.send(self.w.at[pc.f], self.yr.at[d, 0], pc.dev(0, way))
            else:
                self.send(self.part(pc.blk(0, -way), d), self.hr.at[d, 0], pc.dev(0, way))

    def z(self, kh):
        pc = self.pc
        k, h = kh // 10, kh % 10
        if k:
            self.need("z", k, h)
        else:
            self.all_of(0)
        for d, way in ((0, 1), (1, -1)):
            if k + 1 < pc.half or d == h:
                self.send(self.two(-way * k, h), self.zr.at[d, k + 1, h], pc.dev(way, 0))


class PairSum:
    def __init__(self, pc, other, got, mine, came, sems):
        self.pc, self.other, self.got, self.mine, self.came, self.sems = pc, other, got, mine, came, sems

    def swap(self):
        return copy_to(self.other, self.got, self.sems.at[0], self.sems.at[1], self.pc.partner())

    def spread(self):
        pc = self.pc
        for i in range(1, pc.nx):
            x, dev = pc.along_x(i)
            copy_to(self.mine.at[x], self.came.at[pc.x], self.sems.at[2], self.sems.at[3], dev).start()

    def three(self):
        some = self.came.at[pl.ds(0, self.pc.nx - 1)]
        return copy_to(some, some, self.sems.at[2], self.sems.at[3], self.pc.partner())


class PairGather:
    def __init__(self, pc, buf, sems):
        self.pc, self.buf, self.sems = pc, buf, sems

    def own(self):
        pc = self.pc
        ref = self.buf.at[pc.t]
        return copy_to(ref, ref, self.sems.at[2], self.sems.at[3], pc.partner())

    def start(self):
        pc = self.pc
        ref = self.buf.at[pc.t]
        for i in range(1, pc.nx):
            copy_to(ref, ref, self.sems.at[0], self.sems.at[1], pc.along_x(i)[1]).start()
        self.own().start()

    def some(self, i):
        ref = self.buf.at[pl.ds(0, self.pc.nx - 1)]
        return copy_to(ref, ref, self.sems.at[i], self.sems.at[i + 1], self.pc.partner())

    def relay(self):
        pc = self.pc
        self.some(0).wait_recv()
        for i in range(1, pc.nx):
            ref = self.buf.at[pc.along_x(i)[0] * 2 + pc.c]
            copy_to(ref, ref, self.sems.at[4], self.sems.at[5], pc.partner()).start()

    def wait(self):
        self.own().wait_recv()
        self.some(4).wait_recv()

    def drain(self):
        self.some(0).wait_send()
        self.own().wait_send()
        self.some(4).wait_send()


class Exchange:
    def __init__(self, pc, piece, came, sems):
        self.pc, self.piece, self.came, self.sems = pc, piece, came, sems

    def start(self):
        pc, nt = self.pc, self.pc.nx * 2
        for i in range(1, nt):
            to = lax.rem(pc.t + i, nt)
            dst = self.came.at[pc.t]
            copy_to(self.piece(to), dst, self.sems.at[0], self.sems.at[1], (pc.f, to)).start()

    def rest(self):
        some = self.came.at[pl.ds(0, self.pc.nx * 2 - 1)]
        return copy_to(some, some, self.sems.at[0], self.sems.at[1], self.pc.partner())


def nt_dot(a, b):
    return lax.dot_general(a, b, (((1,), (1,)), ((), ())), preferred_element_type=f32)


def turned(column):
    return jnp.broadcast_to(column, (column.shape[0], 128)).T[0:1]


def column_of(row):
    return jnp.broadcast_to(row, (128, row.shape[1])).T


def body(
    nfs, nt,
    tok, mix_gain_in, vw, gw, taps_in, chan_gain_in, ow, mlp_gain_in, uw, dw,
    out,
    mix_gain, taps, chan_gain, mlp_gain,
    x, normed, gb, ob, ub, vb, db, eb,
    padded, conv, stats, hid, mo, mp, mm, mr, nm, resid, aq, ap,
    fx, fp, fm, fr, og,
    load_sem, sems, st_sem, mx_sem, nm_sem, fx_sem, og_sem,
):
    pc = Place(nfs, nt)
    rows, width, tokens = nm.shape[1], x.shape[1], x.shape[0]
    seqs = tokens // LEN
    last = pc.half
    wq, uc, dc = vw.shape[1], ub.shape[2], db.shape[2]
    halves = wq // 128
    reach = taps.shape[0] // 2

    barrier = pltpu.get_barrier_semaphore()
    friends = [pc.dev(dz, 0) for dz in (1, -1, 2, -2)] + [pc.dev(0, dy) for dy in (1, -1, 2)]
    friends += [(pc.f, lax.rem(pc.t + i, nt)) for i in range(1, nt)]
    for dev in friends:
        pl.semaphore_signal(barrier, inc=1, device_id=dev, device_id_type=MESH)

    def load(src, dst, i):
        copy = pltpu.make_async_copy(src, dst, load_sem.at[i])
        copy.start()
        return copy

    own = dict(
        g=[load(vw, gb.at[pc.f, :, pl.ds(0, wq)], 0), load(gw, gb.at[pc.f, :, pl.ds(wq, wq)], 1)],
        o=[load(ow, ob.at[pc.f], 2)],
        u=[load(uw.at[:, pl.ds(0, uc)], ub.at[pc.f], 3)],
        v=[load(uw.at[:, pl.ds(uc, uw.shape[1] - uc)], vb.at[pc.f], 4)],
        d=[load(dw.at[:, pl.ds(0, dc)], db.at[pc.f], 5)],
        e=[load(dw.at[:, pl.ds(dc, dw.shape[1] - dc)], eb.at[pc.f], 6)],
    )
    tok_load = load(tok, x, 7)
    small = [
        load(src, dst, 8 + i)
        for i, (src, dst) in enumerate((
            (mix_gain_in, mix_gain), (taps_in, taps), (chan_gain_in, chan_gain), (mlp_gain_in, mlp_gain),
        ))
    ]

    own["g"][0].wait()
    own["g"].pop(0)
    pl.semaphore_wait(barrier, len(friends))

    stream = {
        name: kind(pc, w, sems[i], own[name], STRIDE.get(name, 1), DIRECT.get(name, last + 1), VIA.get(name, ()))
        for i, (name, kind, w) in enumerate((
            ("g", ZFirst, gb), ("o", ZFirst, ob), ("u", ZFirst, ub), ("v", YFirst, vb), ("d", ZFirst, db),
            ("e", YFirst, eb),
        ))
    }
    part_rows = rows // PARTS
    parts = [pl.ds(i * part_rows, part_rows) for i in range(PARTS)]
    mix_sum = [
        PairSum(pc, mo.at[1 - pc.c, :, p], mp.at[:, p], mm.at[:, p], mr.at[:, p], mx_sem.at[i])
        for i, p in enumerate(parts)
    ]
    norm_all = [PairGather(pc, nm.at[:, p], nm_sem.at[i]) for i, p in enumerate(parts)]
    end = len(GROUPS) - 1
    feed_sum = [PairSum(pc, fx[g].at[1 - pc.c], fp[g], fm[g], fr[g], fx_sem.at[g]) for g in range(end)]
    feed_all = [PairGather(pc, og[g], og_sem.at[g]) for g in range(end)]
    end_sum = Exchange(pc, lambda to: fx[end].at[lax.rem(to, 2), to // 2], fr[end], fx_sem.at[end])
    end_all = Exchange(pc, lambda to: og[end].at[pc.t], og[end], og_sem.at[end])
    stat_all = Exchange(pc, lambda to: stats.at[pc.t], stats, st_sem)

    def norm_in():
        for copy in (tok_load, *small):
            copy.wait()

        def some_rows(i, carry):
            at = pl.ds(pl.multiple_of(i * 32, 32), 32)
            s = x[at].astype(f32)
            scale = lax.rsqrt(jnp.mean(s * s, axis=-1, keepdims=True) + FLOOR)
            normed[at] = (s * scale * mix_gain[...]).astype(bf16)
            return carry

        lax.fori_loop(0, tokens // 32, some_rows, 0)

    def glu():
        for k in range(last + 1):
            stream["g"].all_of(k)
        n_all = normed[...]
        values = jnp.dot(n_all, gb[:, :, pl.ds(0, wq)].reshape(width, wq), preferred_element_type=f32)
        gating = jnp.dot(n_all, gb[:, :, pl.ds(wq, wq)].reshape(width, wq), preferred_element_type=f32)
        glued = (values * jax.nn.sigmoid(gating)).astype(bf16).astype(f32)
        zeros = jnp.zeros((16, 128), f32)
        for h in range(halves):
            for s in range(seqs):
                padded[h, s, pl.ds(0, 16)] = zeros
                padded[h, s, pl.ds(16, LEN)] = glued[s * LEN : (s + 1) * LEN, h * 128 : (h + 1) * 128]
                padded[h, s, pl.ds(16 + LEN, 16)] = zeros

    def convolve():
        for h in range(halves):
            for s in range(seqs):
                total = jnp.zeros((LEN, 128), f32)
                for o in range(taps.shape[0]):
                    tap = taps[pl.ds(o, 1), pl.ds(h * 128, 128)]
                    total = total + padded[h, s, pl.ds(16 - reach + o, LEN)] * tap
                conv[h, pl.ds(s * LEN, LEN)] = total
        sums = sum(jnp.sum(conv[h], axis=-1, keepdims=True) for h in range(halves))
        squares = sum(jnp.sum(conv[h] * conv[h], axis=-1, keepdims=True) for h in range(halves))
        stats[pc.t, pl.ds(0, 1)] = turned(sums)
        stats[pc.t, pl.ds(1, 1)] = turned(squares)
        stat_all.start()

    def mix_rows(core):
        left = hid[:, core].reshape(tokens // 2, wq)
        for c in range(width // 256):
            w = ob[pl.ds(c * 8, 8)].reshape(256, wq)
            mo[core, :, :, pl.ds(c * 256, 256)] = nt_dot(left, w).astype(bf16).reshape(pc.nx, rows, 256)

    def channel_norm():
        stat_all.rest().wait_recv()
        all_stats = jnp.sum(stats[...], axis=0)
        channels = wq * nt
        centre = column_of(all_stats[0:1]) / channels
        spread = column_of(all_stats[1:2]) / channels - centre * centre
        scale = lax.rsqrt(spread + FLOOR)
        for h in range(halves):
            at = pl.ds(h * 128, 128)
            v = (conv[h] - centre) * scale * chan_gain[:, at]
            hid[:, :, :, at] = (v * jax.nn.sigmoid(v)).astype(bf16).reshape(pc.nx, 2, rows, 128)
        for k in range(last + 1):
            stream["o"].all_of(k)
        mix_rows(1 - pc.c)
        for m in mix_sum:
            m.swap().start()

    def mix_pair(i):
        p = parts[i]
        mix_sum[i].swap().wait_recv()
        for j in range(pc.nx):
            mm[j, p] = (mo[pc.c, j, p].astype(f32) + mp[j, p].astype(f32)).astype(bf16)
        mix_sum[i].spread()

    def norm_mid(i):
        p = parts[i]
        mix_sum[i].three().wait_recv()
        mr[pc.x, p] = mm[pc.x, p]
        mixed = sum(mr[j, p].astype(f32) for j in range(pc.nx))
        at = pl.multiple_of(pc.t * rows + i * part_rows, part_rows)
        res = x[pl.ds(at, part_rows)].astype(f32) + mixed.astype(bf16).astype(f32)
        resid[p] = res
        scale = lax.rsqrt(jnp.mean(res * res, axis=-1, keepdims=True) + FLOOR)
        nm[pc.t, p] = (res * scale * mlp_gain[...]).astype(bf16)
        norm_all[i].start()

    def up():
        for n in norm_all:
            n.wait()
        for k in range(last + 1):
            stream["u"].all_of(k)
            stream["v"].all_of(k)
        n_mlp = nm[...].reshape(tokens, width)
        for src, dst in ((ub, aq), (vb, ap)):
            cols = src.shape[2]
            for c in range(0, cols, 256):
                n = min(256, cols - c)
                a = jnp.dot(n_mlp, src[:, :, pl.ds(c, n)].reshape(width, n), preferred_element_type=f32)
                a = jnp.maximum(a, 0.0)
                dst[:, pl.ds(c, n)] = (a * a).astype(bf16)

    def slots(g):
        return [dz for k in GROUPS[g] for dz in pc.shifts(k)]

    def down(g):
        for k in GROUPS[g]:
            stream["d"].all_of(k)
            stream["e"].all_of(k)
        left = jnp.concatenate([aq[...], ap[...]], axis=1)
        for s, dz in enumerate(slots(g)):
            b = pl.ds(pc.row(dz) * NY, NY)
            part = nt_dot(left[:, :dc], db[b].reshape(128, dc))
            part = part + nt_dot(left[:, dc:], eb[b].reshape(128, eb.shape[2]))
            part = part.astype(bf16).reshape(pc.nx, 2, rows, 128)
            for core in range(2):
                fx[g][core, :, :, pl.ds(s * 128, 128)] = part[:, core]
        if g == end:
            end_sum.start()
        else:
            feed_sum[g].swap().start()

    def feed_pair(g):
        feed_sum[g].swap().wait_recv()
        for i in range(pc.nx):
            fm[g][i] = (fx[g][pc.c, i].astype(f32) + fp[g][i].astype(f32)).astype(bf16)
        feed_sum[g].spread()

    def finish(g):
        if g == end:
            end_sum.rest().wait_recv()
            fr[g][pc.t] = fx[g][pc.c, pc.x]
        else:
            feed_sum[g].three().wait_recv()
            fr[g][pc.x] = fm[g][pc.x]
        for s, dz in enumerate(slots(g)):
            at = pl.ds(s * 128, 128)
            feed = sum(fr[g][i, :, at].astype(f32) for i in range(fr[g].shape[0]))
            to = pl.ds(pl.multiple_of(pc.row(dz) * 128, 128), 128)
            og[g][pc.t, :, at] = (resid[:, to] + feed.astype(bf16).astype(f32)).astype(bf16)
        if g == end:
            end_all.start()
        else:
            feed_all[g].start()

    def write(g):
        if g == end:
            end_all.rest().wait_recv()
        else:
            feed_all[g].wait()
        for s, dz in enumerate(slots(g)):
            to = pl.ds(pl.multiple_of(pc.row(dz) * 128, 128), 128)
            out[:, :, to] = og[g][:, :, pl.ds(s * 128, 128)]

    steps = dict(N=norm_in, G=glu, C=convolve, H=channel_norm, I=lambda: mix_rows(pc.c), U=up)
    by_number = dict(
        B=mix_pair, E=norm_mid, L=lambda i: norm_all[i].relay(),
        M=down, S=feed_pair, F=finish, R=lambda g: feed_all[g].relay(), W=write,
    )
    for name in ORDER:
        if "." in name:
            getattr(stream[name[0]], name[2])(int(name[3:]))
        elif name in steps:
            steps[name]()
        else:
            by_number[name[0]](int(name[1:]))

    for s in stream.values():
        s.drain()
    for s in [stat_all, end_sum, end_all]:
        s.rest().wait_send()
    for s in [*mix_sum, *feed_sum]:
        s.swap().wait_send()
        s.three().wait_send()
    for s in [*norm_all, *feed_all]:
        s.drain()


def layer(nfs, nt, tok, mix_gain, vw, gw, taps, chan_gain, ow, mlp_gain, uw, dw):
    tokens, width = tok.shape
    k_rows, wq = vw.shape
    ff = uw.shape[1]
    rows, nx = tokens // nt, nt // 2
    last = nfs // NY // 2
    uc, dc = ff * 5 // 8, ff // 2
    dma = pltpu.SemaphoreType.DMA
    z_first = lambda: [dma(()), dma((2, last + 1)), dma((2, last + 1)), dma((2, last + 1))]
    y_first = lambda: [dma(()), dma((2, last + 1, 2)), dma((2, 1)), dma((2, 1))]
    widths = [sum(1 if k in (0, last) else 2 for k in g) * 128 for g in GROUPS]
    block = lambda c: pltpu.VMEM((nfs, k_rows, c), bf16)
    pairs = lambda w: pltpu.VMEM((2, nx, rows, w), bf16)
    four = lambda w: pltpu.VMEM((nx, rows, w), bf16)
    eight = lambda w: pltpu.VMEM((nt, rows, w), bf16)
    hbm, vmem = pl.BlockSpec(memory_space=pltpu.HBM), pl.BlockSpec(memory_space=pltpu.VMEM)
    scratch = [
        pltpu.VMEM((1, width), f32), pltpu.VMEM(taps.shape, f32), pltpu.VMEM((1, wq), f32), pltpu.VMEM((1, width), f32),
        pltpu.VMEM((tokens, width), bf16),
        pltpu.VMEM((tokens, width), bf16),
        block(2 * wq), block(wq), block(uc), block(ff - uc), block(dc), block(ff - dc),
        pltpu.VMEM((wq // 128, tokens // LEN, LEN + 32, 128), f32),
        pltpu.VMEM((wq // 128, tokens, 128), f32),
        pltpu.VMEM((nt, 2, tokens), f32),
        pltpu.VMEM((nx, 2, rows, wq), bf16),
        pairs(width), four(width), four(width), four(width),
        eight(width),
        pltpu.VMEM((rows, width), f32),
        pltpu.VMEM((tokens, uc), bf16),
        pltpu.VMEM((tokens, ff - uc), bf16),
        [pairs(w) for w in widths], [four(w) for w in widths], [four(w) for w in widths],
        [*(four(w) for w in widths[:-1]), eight(widths[-1])], [eight(w) for w in widths],
        dma((12,)),
        [z_first(), z_first(), z_first(), y_first(), z_first(), y_first()],
        dma((2,)), dma((PARTS, 4)), dma((PARTS, 6)), dma((len(GROUPS), 4)), dma((len(GROUPS), 6)),
    ]
    done = pl.pallas_call(
        functools.partial(body, nfs, nt),
        out_shape=jax.ShapeDtypeStruct((nt, rows, width), bf16),
        in_specs=[hbm] * 10,
        out_specs=vmem,
        scratch_shapes=scratch,
        compiler_params=pltpu.CompilerParams(
            collective_id=0, has_side_effects=True, vmem_limit_bytes=40 * 1024 * 1024
        ),
        name="layer",
    )(
        *(pltpu.with_memory_space_constraint(a, pltpu.HBM) for a in (
            tok, mix_gain.reshape(1, -1), vw, gw, taps, chan_gain.reshape(1, -1), ow.T,
            mlp_gain.reshape(1, -1), uw, dw.T,
        ))
    )
    return done.reshape(tokens, width)


def solution(mesh):
    in_specs = (
        P("fs", None), P(), P("fs", "tp"), P("fs", "tp"), P(None, "tp"),
        P("tp"), P("tp", "fs"), P(), P("fs", "tp"), P("tp", "fs"),
    )
    nfs, nt = mesh.shape["fs"], mesh.shape["tp"]
    return jax.shard_map(
        functools.partial(layer, nfs, nt), mesh=mesh, in_specs=in_specs,
        out_specs=P("fs", None), check_vma=False,
    )
```
